32 devices in a mesh: sp: 4 (over y, x), tp: 8 (over z, core).
Axes of the slice: x: 2, y: 2, z: 4, core: 2. Of those that a mesh axis runs over, the one named last changes fastest.
Arguments:
- queries: bfloat16 [2048, 2048], P('sp', 'tp'), may hold values from -16 to 16
- key_vectors: bfloat16 [2048, 2048], P('sp', 'tp'), may hold values from -4 to 4
- value_vectors: bfloat16 [2048, 2048], P('sp', 'tp'), may hold values from -5 to 5
- forget_totals: float32 [2048, 16], P('sp', 'tp'), may hold values from -344 to 0, as said below
- head_gain: float32 [2048], P('tp'), may hold values from 0.1 to 1.9
- stream: bfloat16 [2048, 2048], P(('sp', 'tp')), may hold values from -6 to 6
- out_weight: bfloat16 [2048, 2048], replicated, may hold values from -0.125 to 0.125
- norm_gain: float32 [2048], replicated, may hold values from 0.1 to 1.9
- routing: int32 [2048, 2], P(('sp', 'tp')), may hold values from 0 to 3, all different within a row; in each aligned block of 64 rows (0 to 63, 64 to 127, ...) at most 64 rows name the same one
- route_weights: float32 [2048, 2], P(('sp', 'tp')), may hold values from 0.2 to 1
- gate_weight: bfloat16 [4, 2048, 4096], P('sp', None, 'tp'), may hold values from -0.125 to 0.125
- up_weight: bfloat16 [4, 2048, 4096], P('sp', None, 'tp'), may hold values from -0.125 to 0.125
- down_weight: bfloat16 [4, 4096, 2048], P('sp', 'tp'), may hold values from -0.09375 to 0.09375
Outputs:
- layer_out: bfloat16 [2048, 2048], P(('sp', 'tp'))
The draws below stay inside these ranges and needn't reach their ends.
Inputs may be any that keep to these rules, and one draw needn't show every extreme that they name: `forget_totals`: along the positions, the values of each head never rise. `routing`: A token's 2 experts differ. Within the tokens of one device (aligned blocks of 64 rows) no expert is named more than 64 times.
All inputs are finite; a program needn't handle non-finite values.
Results may differ from the reference program's by a relative error of at most 0.01145.
Values may be sent and summed in bfloat16 or wider, within the bound.
A program may use at most 128 MiB of HBM per device.

```python
import math
import jax
import jax.numpy as jnp
import numpy as np
from jax import lax

D = 2048
HEAD_COUNT = 16
HD = 128
FF_E = 4096
TOP = 2
TOK_DEV = 512
SEQUENCE_TOKENS = 2048
EXPERTS = 4
ROWS_DEV = 64
CAP = 64
N_TP = 8


def draw_queries(key, part):
    own_key = jax.random.fold_in(key, 11)
    entries = jnp.clip(jax.random.normal(own_key, (SEQUENCE_TOKENS, HEAD_COUNT * HD), jnp.float32), -4.0, 4.0)
    return entries.astype(jnp.bfloat16)


def draw_key_vectors(key, part):
    own_key = jax.random.fold_in(key, 13)
    entries = jnp.clip(jax.random.normal(own_key, (SEQUENCE_TOKENS, HEAD_COUNT * HD), jnp.float32), -4.0, 4.0)
    return entries.astype(jnp.bfloat16)


def draw_forget_totals(key, part):
    ranking = jax.random.permutation(jax.random.fold_in(key, 21), HEAD_COUNT)
    slow_heads = ranking < HEAD_COUNT // 2
    slow_rate = jax.random.uniform(jax.random.fold_in(key, 22), (HEAD_COUNT,), jnp.float32, 0.3, 0.8) / SEQUENCE_TOKENS
    fast_rate = jnp.exp(-jax.random.uniform(jax.random.fold_in(key, 23), (HEAD_COUNT,), jnp.float32, math.log(30.0), math.log(100.0)))
    head_rate = jnp.where(slow_heads, slow_rate, fast_rate)
    block_factor = jnp.exp(jax.random.uniform(jax.random.fold_in(key, 24), (SEQUENCE_TOKENS // TOK_DEV, HEAD_COUNT), jnp.float32, math.log(0.5), math.log(1.5)))
    block_factor = jnp.repeat(block_factor, TOK_DEV, axis=0)
    step_factor = jnp.exp(jax.random.uniform(jax.random.fold_in(key, 25), (SEQUENCE_TOKENS, HEAD_COUNT), jnp.float32, math.log(0.3), math.log(3.0)))
    gate_logarithms = -head_rate[None, :] * block_factor * step_factor
    cluster_positions = jax.random.randint(jax.random.fold_in(key, 26), (3,), 0, SEQUENCE_TOKENS)
    cluster_sizes = jnp.log(jax.random.uniform(jax.random.fold_in(key, 27), (3, HEAD_COUNT), jnp.float32, 0.5, 0.8))
    gate_logarithms = gate_logarithms.at[cluster_positions].add(cluster_sizes)
    return jnp.cumsum(gate_logarithms, axis=0).astype(jnp.float32)


def block_scale(key, dims, shards, least, largest):
    gain = 1.0
    for axis_at, blocks in shards:
        steps = jax.random.uniform(jax.random.fold_in(jax.random.fold_in(key, 6), axis_at), (blocks,), jnp.float32, least / len(shards), largest / len(shards))
        gain = gain * jnp.repeat(jnp.exp(steps), dims[axis_at] // blocks).reshape((-1,) + (1,) * (len(dims) - 1 - axis_at))
    return gain


def routed_block(stream_key, own, number, rows, amount, top, bound, skew):
    sequence = jax.random.permutation(stream_key, amount)
    heavy_load, usual = portions_of(amount, rows * top, bound, skew, True), portions_of(amount, rows * top, bound, skew, False)
    places = jnp.arange(amount)

    def named(lengths, rotation):
        used = int((lengths > 0).sum())
        fixed = max(1, used // 4)
        shifted = fixed + (places - fixed + rotation * (used - fixed)) % max(1, amount - fixed)
        return jnp.zeros((amount,), jnp.int32).at[sequence[jnp.where(places < fixed, places, shifted)]].set(jnp.asarray(lengths, jnp.int32))

    lengths = jnp.where(number % 4 == 0, named(heavy_load, number // 4), named(usual, number - number // 4 - 1))
    mixed = jax.random.permutation(jax.random.fold_in(own, 3), amount)
    donor, receiver = mixed[0:amount // 2 * 2:2], mixed[1:amount // 2 * 2:2]
    slack = jnp.minimum(lengths[donor] - 1, bound - lengths[receiver]) // 2
    slack = jnp.where((donor == sequence[0]) | (receiver == sequence[0]) | (lengths[receiver] == 0), 0, jnp.maximum(slack, 0))
    shifted = jax.random.randint(jax.random.fold_in(own, 4), (amount // 2,), 0, 1 << 20) % (slack + 1)
    lengths = lengths.at[donor].add(-shifted).at[receiver].add(shifted)
    labels = jnp.searchsorted(jnp.cumsum(lengths), jnp.arange(rows * top), side="right").astype(jnp.int32)
    table = labels.reshape(top, rows).T
    table = table[jax.random.permutation(jax.random.fold_in(own, 1), rows)]
    rotation = jax.random.randint(jax.random.fold_in(own, 2), (rows, 1), 0, top)
    return jnp.take_along_axis(table, (jnp.arange(top)[None, :] + rotation) % top, axis=1)


def portions_of(number_of, total, most, slope, full):
    weights = [(1 << 20) // math.isqrt(rank ** slope) + 1 for rank in range(1, number_of + 1)]
    largest = most if full else min(most, max(-(-total // number_of), total * weights[0] // sum(weights)))
    least = 1 if total - largest >= number_of - 1 else 0
    given, spare = [largest] + [least] * (number_of - 1), total - largest - least * (number_of - 1)
    while spare > 0:
        free = [i for i in range(1, number_of) if given[i] < largest] or [i for i in range(1, number_of) if given[i] < most]
        pool, budget = sum([weights[i] for i in free]), spare
        for i in free:
            addition = min(most - given[i], max(1, budget * weights[i] // pool), spare)
            given[i] = given[i] + addition
            spare = spare - addition
    return np.array(given)


def bell_draw(stream_key, dims, spread, bound, split=(), held_as=jnp.bfloat16):
    factor_of = block_scale(stream_key, dims, split, -0.22, 0.18) if split else 1.0
    values = jax.random.normal(stream_key, dims, jnp.float32) * spread * factor_of
    return jnp.minimum(jnp.maximum(values, -bound), bound).astype(held_as)


def setup_inputs(seed: int = 0) -> dict:
    seeds = jax.random.split(jax.random.key(seed), 14)
    queries = draw_queries(jax.random.fold_in(seeds[13], 71), 0)
    key_vectors = draw_key_vectors(jax.random.fold_in(seeds[13], 71), 0)
    value_vectors = bell_draw(seeds[2], (SEQUENCE_TOKENS, HEAD_COUNT * HD), 1.0, 5.0, ((0, 4), (1, 8)))
    forget_totals = draw_forget_totals(jax.random.fold_in(seeds[13], 71), 0)
    head_gain = jnp.clip(1.0 + 0.18 * jax.random.normal(seeds[4], (HEAD_COUNT * HD,), jnp.float32), 0.1, 1.9)
    stream = bell_draw(seeds[5], (SEQUENCE_TOKENS, D), 1.0, 6.0, ((0, 32),))
    out_weight = bell_draw(seeds[6], (HEAD_COUNT * HD, D), (HEAD_COUNT * HD) ** -0.5, 0.125)
    norm_gain = jnp.clip(1.0 + 0.18 * jax.random.normal(seeds[7], (D,), jnp.float32), 0.1, 1.9)
    routing_keys = jax.random.split(jax.random.fold_in(seeds[8], 1), SEQUENCE_TOKENS // ROWS_DEV)
    routing_turns = jax.random.permutation(jax.random.fold_in(seeds[8], 3), SEQUENCE_TOKENS // ROWS_DEV)
    routing = jax.vmap(lambda own, number: routed_block(jax.random.fold_in(seeds[8], 2), own, number, ROWS_DEV, EXPERTS, TOP, CAP, 1))(routing_keys, routing_turns).reshape((SEQUENCE_TOKENS, TOP))
    route_weights = jnp.clip(0.2 + 0.8 * jax.random.uniform(seeds[9], (SEQUENCE_TOKENS, TOP), jnp.float32) ** block_scale(seeds[9], (SEQUENCE_TOKENS, TOP), ((0, 32),), -0.2, 0.2), 0.2, 1.0)
    gate_weight = bell_draw(seeds[10], (EXPERTS, D, FF_E), D ** -0.5, 0.125, ((0, 4), (2, 8)))
    up_weight = bell_draw(seeds[11], (EXPERTS, D, FF_E), D ** -0.5, 0.125, ((0, 4), (2, 8)))
    down_weight = bell_draw(seeds[12], (EXPERTS, FF_E, D), FF_E ** -0.5, 0.09375, ((0, 4), (1, 8)))
    return {"queries": queries, "key_vectors": key_vectors, "value_vectors": value_vectors, "forget_totals": forget_totals, "head_gain": head_gain, "stream": stream, "out_weight": out_weight, "norm_gain": norm_gain, "routing": routing, "route_weights": route_weights, "gate_weight": gate_weight, "up_weight": up_weight, "down_weight": down_weight}


def attention_rows(queries, key_vectors, value_vectors, forget_totals, head_gain):
    seq_len = queries.shape[0]
    query_block = 512 if seq_len % 512 == 0 else seq_len
    query_complete = queries.astype(jnp.float32).reshape(seq_len, HEAD_COUNT, HD)
    key_all = key_vectors.astype(jnp.float32).reshape(seq_len, HEAD_COUNT, HD)
    value_all = value_vectors.astype(jnp.float32).reshape(seq_len, HEAD_COUNT, HD)
    gate_rows = jnp.transpose(forget_totals)
    key_pos = jnp.arange(seq_len, dtype=jnp.int32)
    gain_grid = head_gain.reshape(HEAD_COUNT, 1, HD)

    def one_block(block_index):
        first_row = block_index * query_block
        query_rows = lax.dynamic_slice_in_dim(query_complete, first_row, query_block, 0)
        query_gate = lax.dynamic_slice_in_dim(gate_rows, first_row, query_block, 1)
        scores = jnp.einsum('qhd,khd->hqk', query_rows, key_all) * HD ** (-0.5) + query_gate[:, :, None] - gate_rows[:, None, :]
        query_pos = first_row + jnp.arange(query_block, dtype=jnp.int32)
        visible = (key_pos[None, :] <= query_pos[:, None])[None]
        scores = jnp.where(visible, scores, -jnp.inf)
        row_peak = lax.optimization_barrier(jnp.max(scores, axis=2, keepdims=True))
        lifted = jnp.exp(scores - row_peak)
        row_total = lax.optimization_barrier(jnp.sum(lifted, axis=2))
        rounded = lax.optimization_barrier(lifted.astype(jnp.bfloat16))
        numerator = jnp.einsum('hqk,khd->hqd', rounded.astype(jnp.float32), value_all)
        attended = numerator / row_total[:, :, None]
        inverse_rms = lax.rsqrt(lax.optimization_barrier(jnp.mean(attended * attended, axis=2, keepdims=True)) + 1e-06)
        normed = attended * inverse_rms * gain_grid
        return jnp.transpose(normed, (1, 0, 2)).reshape(query_block, HEAD_COUNT * HD).astype(jnp.bfloat16)
    block_count = seq_len // query_block
    head_out = lax.map(one_block, jnp.arange(block_count, dtype=jnp.int32))
    return head_out.reshape(seq_len, HEAD_COUNT * HD)

def expert_rows(normed_rows, routing, route_weights, gate_weight, up_weight, down_weight):
    token_count = normed_rows.shape[0]
    row_block = 128
    flat_expert = routing.reshape(-1).astype(jnp.int32)
    pair_count = flat_expert.shape[0]
    flat_token = (jnp.arange(pair_count, dtype=jnp.int32) // TOP).astype(jnp.int32)
    flat_weight = route_weights.reshape(-1)
    ordering = jnp.argsort(flat_expert, stable=True)
    sorted_expert = flat_expert[ordering]
    per_expert = lax.optimization_barrier(jnp.sum((flat_expert[:, None] == jnp.arange(EXPERTS, dtype=jnp.int32)[None, :]).astype(jnp.int32), axis=0)).astype(jnp.int32)
    padded = ((per_expert + row_block - 1) // row_block * row_block).astype(jnp.int32)
    pad_end = jnp.cumsum(padded).astype(jnp.int32)
    pad_start = (pad_end - padded).astype(jnp.int32)
    run_start = (jnp.cumsum(per_expert) - per_expert).astype(jnp.int32)
    target = (pad_start[sorted_expert] + jnp.arange(pair_count, dtype=jnp.int32) - run_start[sorted_expert]).astype(jnp.int32)
    block_count = -(-pair_count // row_block) + EXPERTS
    slot_total = block_count * row_block
    slot_token = jnp.full((slot_total,), token_count, jnp.int32).at[target].set(flat_token[ordering])
    slot_weight = jnp.zeros((slot_total,), jnp.float32).at[target].set(flat_weight[ordering])
    block_starts = (jnp.arange(block_count, dtype=jnp.int32) * row_block).astype(jnp.int32)
    block_expert = jnp.minimum(jnp.searchsorted(pad_end, block_starts, side='right').astype(jnp.int32), EXPERTS - 1).astype(jnp.int32)
    padded_rows = jnp.concatenate([normed_rows, jnp.zeros((1, normed_rows.shape[1]), normed_rows.dtype)], axis=0)[slot_token]
    units_dev = FF_E // N_TP

    def expert_block(block_args):
        block_in, expert_id = block_args
        gate_pre = jnp.dot(block_in, gate_weight[expert_id], preferred_element_type=jnp.float32)
        up_pre = jnp.dot(block_in, up_weight[expert_id], preferred_element_type=jnp.float32)
        hidden = lax.optimization_barrier((jax.nn.silu(gate_pre) * up_pre).astype(jnp.bfloat16))
        grouped_rows = jnp.transpose(hidden.reshape(row_block, N_TP, units_dev), (1, 0, 2)).astype(jnp.float32)
        down_groups = down_weight[expert_id].reshape(N_TP, units_dev, -1).astype(jnp.float32)
        partial_value = lax.optimization_barrier(jnp.einsum('gbf,gfd->gbd', grouped_rows, down_groups).astype(jnp.bfloat16))
        return lax.optimization_barrier(jnp.sum(partial_value.astype(jnp.float32), axis=0)).astype(jnp.bfloat16)
    expert_out = lax.map(expert_block, (padded_rows.reshape(block_count, row_block, -1), block_expert))
    expert_out = expert_out.reshape(slot_total, -1)
    weighted = expert_out.astype(jnp.float32) * slot_weight[:, None]
    return jax.ops.segment_sum(weighted, slot_token, num_segments=token_count + 1)[:token_count]

def reference(queries, key_vectors, value_vectors, forget_totals, head_gain, stream, out_weight, norm_gain, routing, route_weights, gate_weight, up_weight, down_weight):
    head_out = attention_rows(queries, key_vectors, value_vectors, forget_totals, head_gain)
    mixed_rows = jnp.dot(head_out, out_weight, preferred_element_type=jnp.float32)
    resid_sum = stream.astype(jnp.float32) + mixed_rows
    center = resid_sum - lax.optimization_barrier(jnp.mean(resid_sum, axis=1, keepdims=True))
    normed_rows = (center * lax.rsqrt(lax.optimization_barrier(jnp.mean(center * center, axis=1, keepdims=True)) + 1e-05) * norm_gain).astype(jnp.bfloat16)
    routed = expert_rows(normed_rows, routing, route_weights, gate_weight, up_weight, down_weight)
    return (resid_sum + routed).astype(jnp.bfloat16)
```

```python
from functools import partial

import jax
import jax.numpy as jnp
from jax import lax
from jax.experimental import pallas as pl
from jax.experimental.pallas import tpu as pltpu
from jax.sharding import PartitionSpec as P

HD = 128
TOP = 2


masked_score = -1e30


def attend_block(
    totals, query_rows, query_gate, query_pos, key_rows, value_rows, key_gate, key_pos
):
    run_max, run_sum, run_acc = totals
    scores = jnp.einsum("qhd,khd->hqk", query_rows, key_rows, preferred_element_type=jnp.float32)
    scores = scores * HD ** (-0.5) + query_gate[:, :, None] - key_gate[:, None, :]
    visible = (key_pos[None, :] <= query_pos[:, None])[None]
    scores = jnp.where(visible, scores, masked_score)
    new_max = jnp.maximum(run_max, jnp.max(scores, axis=2))
    lifted = jnp.where(visible, jnp.exp(scores - new_max[:, :, None]), 0.0)
    rescale = jnp.exp(run_max - new_max)
    new_sum = run_sum * rescale + jnp.sum(lifted, axis=2)
    product = jnp.einsum(
        "hqk,khd->hqd", lifted.astype(jnp.bfloat16), value_rows, preferred_element_type=jnp.float32
    )
    new_acc = run_acc * rescale[:, :, None] + product
    return (new_max, new_sum, new_acc)


def keep_totals(totals_in):
    return totals_in


def make_folder(segments, gathered_gates):

    def fold_keys(state_all, key_piece, first_key):
        key_part, value_part = key_piece
        key_total = key_part.shape[0]
        block_len = min(512, key_total)
        heads_dev = segments[0][0].shape[1]
        key_part = key_part.reshape(key_total, heads_dev, HD)
        value_part = value_part.reshape(key_total, heads_dev, HD)

        def one_block(block_index, state_now):
            offset = block_index * block_len
            key_rows = lax.dynamic_slice_in_dim(key_part, offset, block_len, 0)
            value_rows = lax.dynamic_slice_in_dim(value_part, offset, block_len, 0)
            key_pos = offset + jnp.arange(block_len, dtype=jnp.int32)
            key_gate = jnp.transpose(lax.dynamic_slice_in_dim(gathered_gates, offset, block_len, 0))
            updated = []
            for segment, totals_in in zip(segments, state_now):
                query_rows, query_gate, query_pos = segment
                needed = offset <= query_pos[-1]
                advance = partial(
                    attend_block,
                    query_rows=query_rows,
                    query_gate=query_gate,
                    query_pos=query_pos,
                    key_rows=key_rows,
                    value_rows=value_rows,
                    key_gate=key_gate,
                    key_pos=key_pos,
                )
                updated.append(lax.cond(needed, advance, keep_totals, totals_in))
            return tuple(updated)

        return lax.fori_loop(0, key_total // block_len, one_block, state_all)

    return fold_keys


MESH = pl.DeviceIdType.MESH
LANES = 128
QUADS = 4
LOG2E = 1.4426950408889634

TASKS = (
    ("far", 0),
    ("zar", 1),
    ("zar", 2),
    ("s", 0),
    ("f", 0),
    ("far", 1),
    ("co", 0),
    ("zar", 3),
    ("cp", 0),
    ("far", 2),
    ("s", 1),
    ("f", 1),
    ("co", 1),
    ("far", 3),
    ("r1", 0),
    ("cp", 1),
    ("s", 2),
    ("f", 2),
    ("co", 2),
    ("r1", 1),
    ("cp", 2),
    ("r1", 2),
    ("s", 3),
    ("f", 3),
    ("co", 3),
    ("cp", 3),
    ("r2", 1),
    ("r3", 1),
    ("r1", 3),
    ("r2", 2),
    ("r3", 2),
    ("r2", 3),
    ("r3", 3),
    ("r2", 0),
    ("r3", 0),
)


def layer_kernel(
    depth,
    queries_hbm,
    keys_hbm,
    values_hbm,
    gates_hbm,
    gain_hbm,
    stream_hbm,
    out_hbm,
    norm_hbm,
    routing_hbm,
    route_hbm,
    gate_hbm,
    up_hbm,
    down_hbm,
    out_ref,
    queries,
    stream,
    gain,
    norm_gain,
    routing,
    route_w,
    key_all,
    value_all,
    gate_all,
    weights_all,
    wcols,
    qcol,
    peak,
    weight_total,
    weighted,
    leaving,
    incoming,
    resid,
    out_w,
    rows_all,
    gate_w,
    up_w,
    down_w,
    hidden,
    mine,
    theirs,
    from_core,
    from_second,
    from_first,
    from_z,
    from_zf,
    local_sems,
    kv_send_sems,
    kv_recv_sems,
    out_send_sems,
    out_recv_sems,
    w_send_sems,
    w_recv_sems,
    wq_recv_sems,
    ag_send_sems,
    ag_recv_sems,
    rs_send_sems,
    core_sems,
    second_sems,
    first_sems,
    z_sems,
    zf_sems,
):
    sp = lax.axis_index("sp")
    tp = lax.axis_index("tp")
    tp_count = 2 * depth
    tokens = queries.shape[0]
    heads = queries.shape[1] // HD
    count, width = resid.shape
    units = gate_w.shape[1]
    z, core = tp // 2, tp % 2
    other = 1 - core
    x_next = sp + 1 - 2 * (sp % 2)
    y_next = (sp + 2) % 4
    first = x_next * (1 - core) + y_next * core
    second = y_next * (1 - core) + x_next * core
    far = 3 - sp
    to_core = (sp, z * 2 + other)
    to_first = (first, tp)
    to_second = (second, tp)

    def f32(value):
        return value.astype(jnp.float32)

    def bf16(value):
        return value.astype(jnp.bfloat16)

    def at_z(level):
        return (sp, level * 2 + core)

    orders = []
    for at in range(depth):
        order = [at]
        for step in range(1, depth):
            order += [lev for lev in (at - step, at + step) if 0 <= lev < depth]
        orders.append(order)
    levels = []
    for place in range(depth):
        total = 0
        for at in range(depth):
            apart = (z - at + depth) % depth
            total = total + orders[at][place] * (1 - (apart + depth - 1) // depth)
        levels.append(total)

    def adjacent(level):
        return (level - z) * (level - z) == 1

    loads = {}

    def load(name, src, dst):
        loads[name] = pltpu.make_async_copy(src, dst, local_sems.at[len(loads)])
        loads[name].start()

    load("keys", keys_hbm, key_all.at[sp])
    load("values", values_hbm, value_all.at[sp])
    load("gates", gates_hbm, gate_all.at[sp])
    load("queries", queries_hbm, queries)
    load("routing", routing_hbm, routing)
    load("route", route_hbm, route_w)

    barrier = pltpu.get_barrier_semaphore()
    peers = [to_first, to_second]
    peers += [(sp, (tp + step) % tp_count) for step in range(1, tp_count)]
    for peer in peers:
        pl.semaphore_signal(barrier, inc=1, device_id=peer, device_id_type=MESH)
    pl.semaphore_wait(barrier, len(peers))

    sent = []

    def send(src, dst, send_sem, recv_sem, target, when=None):
        copy = pltpu.make_async_remote_copy(
            src_ref=src,
            dst_ref=dst,
            send_sem=send_sem,
            recv_sem=recv_sem,
            device_id=target,
            device_id_type=MESH,
        )
        if when is None:
            copy.start()
        else:
            pl.when(when)(copy.start)
        sent.append((copy, when))

    def landed(dst, sem):
        pltpu.make_async_remote_copy(
            src_ref=dst,
            dst_ref=dst,
            send_sem=kv_send_sems.at[0],
            recv_sem=sem,
            device_id=to_core,
            device_id_type=MESH,
        ).wait_recv()

    kv_refs = (key_all, value_all, gate_all)
    kv_count = [0]

    def kv_send(quad, part, target):
        ref = kv_refs[part].at[quad]
        send(ref, ref, kv_send_sems.at[kv_count[0]], kv_recv_sems.at[quad, part], target)
        kv_count[0] += 1

    def kv_landed(quad, part):
        landed(kv_refs[part].at[quad], kv_recv_sems.at[quad, part])

    for part, name in enumerate(("keys", "values", "gates")):
        loads[name].wait()
        kv_send(sp, part, to_first)
        kv_send(sp, part, to_second)
    load("stream", stream_hbm, stream)
    load("gain", gain_hbm, gain)
    load("norm", norm_hbm, norm_gain)
    load("out", out_hbm, out_w)
    load("gate", gate_hbm.at[0], gate_w)
    load("up", up_hbm.at[0], up_w)
    load("down", down_hbm.at[0], down_w)

    for name in ("routing", "route", "queries"):
        loads[name].wait()
    own_weights = weights_all.at[sp, tp]
    own_weights[...] = jnp.zeros_like(own_weights)
    for expert in range(QUADS):
        row = 0.0
        for k in range(routing.shape[0]):
            row = row + jnp.where(
                routing[k : k + 1, :] == expert, route_w[k : k + 1, :], 0.0
            )
        own_weights[expert : expert + 1, :count] = row

    chunk = LANES
    for head in range(heads):
        for at in range(tokens // chunk):
            span = slice(at * chunk, (at + 1) * chunk)
            row = gate_all[sp, head : head + 1, span] * LOG2E
            qcol[head, span] = jnp.transpose(jnp.broadcast_to(row, (chunk, chunk)))[:, :1]

    def attend(quad, diagonal):
        @pl.loop(0, tokens // chunk)
        def _(j):
            rows = pl.ds(pl.multiple_of(j * chunk, chunk), chunk)
            for head in range(heads):
                cols = slice(head * HD, (head + 1) * HD)
                scores = lax.dot_general(
                    queries[rows, cols],
                    key_all[quad, :, cols],
                    (((1,), (1,)), ((), ())),
                    preferred_element_type=jnp.float32,
                )
                query_gate = qcol[head, rows]
                key_gate = gate_all[quad, head : head + 1, :] * LOG2E
                scores = scores * (HD ** (-0.5) * LOG2E) - key_gate
                if diagonal:
                    row_id = lax.broadcasted_iota(jnp.int32, scores.shape, 0) + j * chunk
                    col_id = lax.broadcasted_iota(jnp.int32, scores.shape, 1)
                    scores = jnp.where(col_id <= row_id, scores, masked_score)
                new_peak = jnp.max(scores, axis=1, keepdims=True) + query_gate
                if not diagonal:
                    old_peak = peak[head, rows]
                    new_peak = jnp.maximum(old_peak, new_peak)
                lifted = jnp.exp2(scores + (query_gate - new_peak))
                added = jnp.sum(lifted, axis=1, keepdims=True)
                product = jnp.dot(
                    lifted.astype(jnp.bfloat16),
                    value_all[quad, :, cols],
                    preferred_element_type=jnp.float32,
                )
                if not diagonal:
                    rescale = jnp.exp2(old_peak - new_peak)
                    added = weight_total[head, rows] * rescale + added
                    product = weighted[head, rows] * rescale + product
                peak[head, rows] = new_peak
                weight_total[head, rows] = added
                weighted[head, rows] = product

    def attend_earlier(quad):
        @pl.when(quad < sp)
        def _():
            attend(quad, False)

    attend(sp, True)
    for step in range(1, tp_count):
        target = (tp + step) % tp_count
        ref = weights_all.at[sp, tp]
        send(ref, ref, w_send_sems.at[step], w_recv_sems.at[tp], (sp, target))
    for part in range(3):
        kv_landed(first, part)
        kv_send(first, part, to_second)
    attend_earlier(first)
    for part in range(3):
        kv_landed(second, part)
    attend_earlier(second)
    for step in range(1, tp_count):
        source = (tp + step) % tp_count
        landed(weights_all.at[sp, source], w_recv_sems.at[source])
    for part in range(3):
        kv_landed(far, part)
    attend_earlier(far)

    loads["gain"].wait()

    @pl.loop(0, tp_count)
    def _(j):
        rows = pl.ds(pl.multiple_of(j * count, count), count)
        for head in range(heads):
            cols = slice(head * HD, (head + 1) * HD)
            attended = weighted[head, rows] / weight_total[head, rows]
            square = jnp.mean(attended * attended, axis=1, keepdims=True)
            normed = attended * lax.rsqrt(square + 1e-06) * gain[0:1, cols]
            leaving[j, :, cols] = normed.astype(jnp.bfloat16)

    for at, level in enumerate(reversed(levels)):
        for side in (core, other):
            if at == depth - 1 and side is core:
                continue
            target = level * 2 + side
            index = 2 * at + (0 if side is core else 1)
            send(
                leaving.at[target],
                incoming.at[tp],
                out_send_sems.at[index],
                out_recv_sems.at[tp],
                (sp, target),
            )

    send(weights_all.at[sp], weights_all.at[sp], w_send_sems.at[0], wq_recv_sems.at[sp], to_first)
    send(
        weights_all.at[sp],
        weights_all.at[sp],
        w_send_sems.at[tp_count],
        wq_recv_sems.at[sp],
        to_second,
    )
    loads["stream"].wait()
    resid[...] = f32(stream[...])
    loads["out"].wait()
    loads["norm"].wait()
    landed(weights_all.at[first], wq_recv_sems.at[first])
    send(
        weights_all.at[first],
        weights_all.at[first],
        w_send_sems.at[tp_count + 1],
        wq_recv_sems.at[first],
        to_second,
    )
    wide = heads * HD
    strip = 512 if width % 512 == 0 else width
    for at, level in enumerate(levels):
        for side in (core, other):
            source = level * 2 + side
            own = at == 0 and side is core
            part = leaving if own else incoming
            if not own:
                landed(incoming.at[source], out_recv_sems.at[source])

            @pl.loop(0, width // strip)
            def _(j, part=part, source=source):
                cols = pl.ds(pl.multiple_of(j * strip, strip), strip)
                weights = out_w[pl.ds(pl.multiple_of(source * wide, wide), wide), cols]
                resid[:, cols] += jnp.dot(
                    part[source], weights, preferred_element_type=jnp.float32
                )

    total = resid[...]
    center = total - jnp.mean(total, axis=1, keepdims=True)
    variance = jnp.mean(center * center, axis=1, keepdims=True)
    rows_all[core, z, sp] = (center * lax.rsqrt(variance + 1e-05) * norm_gain[0:1, :]).astype(
        jnp.bfloat16
    )

    ag_count = [0]

    def spread(level, quad, target, when=None):
        ref = rows_all.at[core, level, quad]
        sem = ag_recv_sems.at[core, level, quad]
        send(ref, ref, ag_send_sems.at[ag_count[0]], sem, target, when)
        ag_count[0] += 1

    def arrived(half, level, quad):
        landed(rows_all.at[half, level, quad], ag_recv_sems.at[half, level, quad])

    above, below = at_z((z + 1) % depth), at_z((z + depth - 1) % depth)
    spread(z, sp, above, z < depth - 1)
    spread(z, sp, below, z > 0)
    for target in (to_first, to_second, to_core):
        spread(z, sp, target)

    landed(weights_all.at[second], wq_recv_sems.at[second])
    landed(weights_all.at[far], wq_recv_sems.at[far])
    lane = lax.broadcasted_iota(jnp.int32, (QUADS, LANES), 0)
    picked = []
    for quad in range(QUADS):
        for source in range(tp_count):
            tile = weights_all[quad, source]
            picked.append(jnp.sum(jnp.where(lane == sp, tile, 0.0), axis=0, keepdims=True))
    fill = jnp.zeros((LANES - len(picked), LANES), jnp.float32)
    turned = jnp.transpose(jnp.concatenate(picked + [fill], axis=0))
    for quad in range(QUADS):
        for source in range(tp_count):
            at = quad * tp_count + source
            wcols[source % 2, source // 2, quad] = turned[:count, at : at + 1]

    for name in ("gate", "up", "down"):
        loads[name].wait()

    def experts(half, level, dest):
        piece = 256 if units % 256 == 0 else units

        @pl.loop(0, units // piece)
        def _(j):
            cols = pl.ds(pl.multiple_of(j * piece, piece), piece)
            block = rows_all[half, level].reshape(QUADS * count, width)
            gate_pre = jnp.dot(block, gate_w[:, cols], preferred_element_type=jnp.float32)
            up_pre = jnp.dot(block, up_w[:, cols], preferred_element_type=jnp.float32)
            hidden[:, cols] = (gate_pre / (1.0 + jnp.exp(-gate_pre)) * up_pre).astype(jnp.bfloat16)

        @pl.loop(0, width // strip)
        def _(j):
            cols = pl.ds(pl.multiple_of(j * strip, strip), strip)
            weight = wcols[half, level].reshape(QUADS * count, 1)
            product = jnp.dot(hidden[...], down_w[:, cols], preferred_element_type=jnp.float32)
            dest[level, :, :, cols] = bf16(product * weight).reshape(QUADS, count, strip)

    rs_count = [0]

    def send_back(src, dst, sem, target, when=None):
        send(src, dst, rs_send_sems.at[rs_count[0]], sem, target, when)
        rs_count[0] += 1

    def from_z_near(place):
        level = levels[place]
        arrived(core, level, sp)
        spread(level, sp, above, (level < z) & (z < depth - 1))
        spread(level, sp, below, (level > z) & (z > 0))
        spread(level, sp, to_first, (level - z) * (level - z) != 1)
        spread(level, sp, to_second)
        spread(level, sp, to_core)

    def from_first_near(place):
        level = levels[place]
        arrived(core, level, first)
        if place == 0:
            spread(level, first, above, z < depth - 1)
            spread(level, first, below, z > 0)
        spread(level, first, to_second)
        spread(level, first, to_core)

    def from_second_near(place):
        arrived(core, levels[place], second)
        spread(levels[place], second, to_core)

    def from_far(place):
        arrived(core, levels[place], far)
        spread(levels[place], far, to_core)

    def own_half(place):
        experts(core, levels[place], mine)

    def partner_half(place):
        level = levels[place]
        for quad in range(QUADS):
            arrived(other, level, quad)
        experts(other, level, theirs)
        send_back(theirs.at[level], from_core.at[level], core_sems.at[level], to_core)

    def both_halves(place):
        level = levels[place]
        landed(from_core.at[level], core_sems.at[level])
        for slot, quad in ((1, far), (0, second)):
            mine[level, quad] = bf16(f32(mine[level, quad]) + f32(from_core[level, quad]))
            send_back(
                mine.at[level, quad],
                from_second.at[level, slot],
                second_sems.at[level, slot],
                to_second,
            )

    def onto_first(place):
        level = levels[place]
        landed(from_second.at[level, 1], second_sems.at[level, 1])
        if place == 0:
            for near in levels[1:]:

                @pl.when(adjacent(near))
                def _(near=near):
                    landed(from_zf.at[near], zf_sems.at[near])
                    mine[z, first] = bf16(f32(mine[z, first]) + f32(from_zf[near]))

        mine[level, first] = bf16(
            f32(mine[level, first]) + f32(from_core[level, first]) + f32(from_second[level, 1])
        )
        src = mine.at[level, first]
        if place:
            near = adjacent(level)
            send_back(src, from_zf.at[z], zf_sems.at[z], at_z(level), near)
            apart = (level - z) * (level - z) != 1
            send_back(src, from_first.at[level], first_sems.at[level], to_first, apart)
        else:
            send_back(src, from_first.at[level], first_sems.at[level], to_first)

    def onto_owner(place):
        level = levels[place]
        landed(from_second.at[level, 0], second_sems.at[level, 0])
        if place:

            @pl.when((level - z) * (level - z) != 1)
            def _():
                landed(from_first.at[level], first_sems.at[level])
                mine[level, sp] = bf16(
                    f32(mine[level, sp])
                    + f32(from_core[level, sp])
                    + f32(from_second[level, 0])
                    + f32(from_first[level])
                )

            @pl.when(adjacent(level))
            def _():
                mine[level, sp] = bf16(
                    f32(mine[level, sp])
                    + f32(from_core[level, sp])
                    + f32(from_second[level, 0])
                )

            send_back(mine.at[level, sp], from_z.at[z], z_sems.at[z], at_z(level))
        else:
            landed(from_first.at[level], first_sems.at[level])
            resid[...] += (
                f32(mine[level, sp])
                + f32(from_core[level, sp])
                + f32(from_second[level, 0])
                + f32(from_first[level])
            )

    tasks = dict(
        zar=from_z_near,
        far=from_first_near,
        s=from_second_near,
        f=from_far,
        co=own_half,
        cp=partner_half,
        r1=both_halves,
        r2=onto_first,
        r3=onto_owner,
    )
    for name, place in TASKS:
        tasks[name](place)

    total = resid[...]
    for near in levels[1:]:
        landed(from_z.at[near], z_sems.at[near])
        total = total + f32(from_z[near])
    out_ref[...] = total.astype(out_ref.dtype)
    for copy, when in sent:
        if when is None:
            copy.wait_send()
        else:
            pl.when(when)(copy.wait_send)


def whole_layer(
    queries,
    keys,
    values,
    forget_totals,
    head_gain,
    stream,
    out_weight,
    norm_gain,
    routing,
    route_weights,
    gate_weight,
    up_weight,
    down_weight,
):
    tokens, wide = queries.shape
    heads = wide // HD
    count, width = stream.shape
    units = gate_weight.shape[2]
    tp_count = lax.axis_size("tp")
    depth = tp_count // 2
    top = routing.shape[1]
    bf16, f32 = jnp.bfloat16, jnp.float32
    dma = pltpu.SemaphoreType.DMA
    vmem = pltpu.VMEM
    plane = (depth, QUADS, count, width)
    hbm = pl.BlockSpec(memory_space=pltpu.HBM)
    ag_sends = 5 + 5 * (depth - 1) + 2 * depth + 2 + 2 * depth
    rs_sends = depth + 2 * depth + 2 * depth + depth
    return pl.pallas_call(
        partial(layer_kernel, depth),
        out_shape=jax.ShapeDtypeStruct((count, width), bf16),
        in_specs=[hbm] * 13,
        out_specs=pl.BlockSpec(memory_space=pltpu.VMEM),
        scratch_shapes=[
            vmem((tokens, wide), bf16),
            vmem((count, width), bf16),
            vmem((1, wide), f32),
            vmem((1, width), f32),
            vmem((top, count), jnp.int32),
            vmem((top, count), f32),
            vmem((QUADS, tokens, wide), bf16),
            vmem((QUADS, tokens, wide), bf16),
            vmem((QUADS, heads, tokens), f32),
            vmem((QUADS, tp_count, QUADS, LANES), f32),
            vmem((2, depth, QUADS, count, 1), f32),
            vmem((heads, tokens, 1), f32),
            vmem((heads, tokens, 1), f32),
            vmem((heads, tokens, 1), f32),
            vmem((heads, tokens, HD), f32),
            vmem((tp_count, count, wide), bf16),
            vmem((tp_count, count, wide), bf16),
            vmem((count, width), f32),
            vmem(out_weight.shape, bf16),
            vmem((2,) + plane, bf16),
            vmem((width, units), bf16),
            vmem((width, units), bf16),
            vmem((units, width), bf16),
            vmem((QUADS * count, units), bf16),
            vmem(plane, bf16),
            vmem(plane, bf16),
            vmem(plane, bf16),
            vmem((depth, 2, count, width), bf16),
            vmem((depth, count, width), bf16),
            vmem((depth, count, width), bf16),
            vmem((depth, count, width), bf16),
            dma((13,)),
            dma((9,)),
            dma((QUADS, 3)),
            dma((tp_count,)),
            dma((tp_count,)),
            dma((tp_count + 2,)),
            dma((tp_count,)),
            dma((QUADS,)),
            dma((ag_sends,)),
            dma((2, depth, QUADS)),
            dma((rs_sends,)),
            dma((depth,)),
            dma((depth, 2)),
            dma((depth,)),
            dma((depth,)),
            dma((depth,)),
        ],
        compiler_params=pltpu.CompilerParams(
            collective_id=0, has_side_effects=True, vmem_limit_bytes=58 * 2**20
        ),
    )(
        queries,
        keys,
        values,
        jnp.transpose(forget_totals),
        head_gain.reshape(1, -1),
        stream,
        out_weight,
        norm_gain.reshape(1, -1),
        jnp.transpose(routing),
        jnp.transpose(route_weights),
        gate_weight,
        up_weight,
        down_weight,
    )


def routed_experts(
    resid_sum, normed_rows, routing, route_weights, gate_weight, up_weight, down_weight
):
    sp_count = lax.axis_size("sp")
    row_count = normed_rows.shape[0]
    capacity = max(2, 2 * TOP * row_count // sp_count)
    flat_expert = routing.reshape(-1)
    onehot = (flat_expert[:, None] == jnp.arange(sp_count, dtype=jnp.int32)[None, :]).astype(
        jnp.int32
    )
    earlier = jnp.cumsum(onehot, axis=0) - onehot
    slot_index = flat_expert * capacity + jnp.sum(earlier * onehot, axis=1)
    slot_grid = slot_index.reshape(row_count, TOP)
    slot_ids = jnp.arange(sp_count * capacity, dtype=jnp.int32)
    placing = jnp.sum(
        (slot_grid[None, :, :] == slot_ids[:, None, None]).astype(jnp.float32), axis=2
    ).astype(jnp.bfloat16)
    outgoing = jnp.dot(placing, normed_rows, preferred_element_type=jnp.float32).astype(
        jnp.bfloat16
    )
    outgoing = outgoing.reshape(sp_count, capacity, normed_rows.shape[1])
    arrived = lax.all_to_all(outgoing, "sp", split_axis=0, concat_axis=0, tiled=True)
    row_piece = lax.all_gather(arrived.reshape(-1, arrived.shape[2]), "tp", axis=0, tiled=True)
    gate_pre = jnp.dot(row_piece, gate_weight[0], preferred_element_type=jnp.float32)
    up_pre = jnp.dot(row_piece, up_weight[0], preferred_element_type=jnp.float32)
    hidden = (jax.nn.silu(gate_pre) * up_pre).astype(jnp.bfloat16)
    summed = lax.psum_scatter(
        jnp.dot(hidden, down_weight[0], preferred_element_type=jnp.float32).astype(jnp.bfloat16),
        "tp",
        scatter_dimension=0,
        tiled=True,
    )
    expert_out = summed.reshape(sp_count, capacity, -1)
    returned = lax.all_to_all(expert_out, "sp", split_axis=0, concat_axis=0, tiled=True)
    picked = returned.reshape(sp_count * capacity, -1)[slot_index].astype(jnp.float32)
    weighted = picked * route_weights.reshape(-1)[:, None]
    routed = jnp.sum(weighted.reshape(row_count, TOP, -1), axis=1)
    return (resid_sum + routed).astype(jnp.bfloat16)


def on_device(
    queries,
    key_vectors,
    value_vectors,
    forget_totals,
    head_gain,
    stream,
    out_weight,
    norm_gain,
    routing,
    route_weights,
    gate_weight,
    up_weight,
    down_weight,
):
    rows_dev, sp_size, tp_size = stream.shape[0], lax.axis_size("sp"), lax.axis_size("tp")
    dense = 2 * TOP * rows_dev // sp_size >= rows_dev
    leveled = sp_size == QUADS and tp_size == 2 * len({place for _, place in TASKS})
    if dense and leveled and queries.shape[0] % LANES == 0 and rows_dev <= LANES:
        return whole_layer(
            queries,
            key_vectors,
            value_vectors,
            forget_totals,
            head_gain,
            stream,
            out_weight,
            norm_gain,
            routing,
            route_weights,
            gate_weight,
            up_weight,
            down_weight,
        )
    tok_count = queries.shape[0]
    heads_dev = queries.shape[1] // HD
    sp_index = lax.axis_index("sp")
    sp_count = lax.axis_size("sp")
    gathered_gates = lax.all_gather(forget_totals, "sp", axis=0, tiled=True)
    first_pos = sp_index * tok_count
    query_pos = first_pos + jnp.arange(tok_count, dtype=jnp.int32)
    query_gate = jnp.transpose(lax.dynamic_slice_in_dim(gathered_gates, first_pos, tok_count, 0))
    segments = [(queries.reshape(tok_count, heads_dev, HD), query_gate, query_pos)]
    starting = (
        (
            jnp.full((heads_dev, tok_count), masked_score, jnp.float32),
            jnp.zeros((heads_dev, tok_count), jnp.float32),
            jnp.zeros((heads_dev, tok_count, HD), jnp.float32),
        ),
    )
    folder = make_folder(segments, gathered_gates)
    totals = folder(
        starting,
        (
            lax.all_gather(key_vectors, "sp", axis=0, tiled=True),
            lax.all_gather(value_vectors, "sp", axis=0, tiled=True),
        ),
        jnp.int32(0),
    )
    run_max, run_sum, run_acc = totals[0]
    attended = run_acc / run_sum[:, :, None]
    inverse_rms = lax.rsqrt(jnp.mean(attended * attended, axis=2, keepdims=True) + 1e-06)
    normed = attended * inverse_rms * head_gain.reshape(heads_dev, 1, HD)
    head_out = (
        jnp.transpose(normed, (1, 0, 2)).reshape(tok_count, heads_dev * HD).astype(jnp.bfloat16)
    )
    token_heads = lax.all_to_all(head_out, "tp", split_axis=0, concat_axis=1, tiled=True)
    mixed_rows = jnp.dot(token_heads, out_weight, preferred_element_type=jnp.float32)
    resid_sum = stream.astype(jnp.float32) + mixed_rows
    center = resid_sum - jnp.mean(resid_sum, axis=1, keepdims=True)
    normed_rows = (
        center * lax.rsqrt(jnp.mean(center * center, axis=1, keepdims=True) + 1e-05) * norm_gain
    ).astype(jnp.bfloat16)
    return routed_experts(
        resid_sum, normed_rows, routing, route_weights, gate_weight, up_weight, down_weight
    )


def solution(mesh):
    in_specs = (
        P("sp", "tp"),
        P("sp", "tp"),
        P("sp", "tp"),
        P("sp", "tp"),
        P("tp"),
        P(("sp", "tp"), None),
        P(),
        P(),
        P(("sp", "tp"), None),
        P(("sp", "tp"), None),
        P("sp", None, "tp"),
        P("sp", None, "tp"),
        P("sp", "tp", None),
    )
    out_specs = P(("sp", "tp"), None)
    return jax.shard_map(
        on_device, mesh=mesh, in_specs=in_specs, out_specs=out_specs, check_vma=False
    )
```

```python
from functools import partial

import jax
import jax.numpy as jnp
from jax import lax
from jax.experimental import pallas as pl
from jax.experimental.pallas import tpu as pltpu
from jax.sharding import PartitionSpec as P

HD = 128
TOP = 2


masked_score = -1e30


def attend_block(
    totals, query_rows, query_gate, query_pos, key_rows, value_rows, key_gate, key_pos
):
    run_max, run_sum, run_acc = totals
    scores = jnp.einsum("qhd,khd->hqk", query_rows, key_rows, preferred_element_type=jnp.float32)
    scores = scores * HD ** (-0.5) + query_gate[:, :, None] - key_gate[:, None, :]
    visible = (key_pos[None, :] <= query_pos[:, None])[None]
    scores = jnp.where(visible, scores, masked_score)
    new_max = jnp.maximum(run_max, jnp.max(scores, axis=2))
    lifted = jnp.where(visible, jnp.exp(scores - new_max[:, :, None]), 0.0)
    rescale = jnp.exp(run_max - new_max)
    new_sum = run_sum * rescale + jnp.sum(lifted, axis=2)
    product = jnp.einsum(
        "hqk,khd->hqd", lifted.astype(jnp.bfloat16), value_rows, preferred_element_type=jnp.float32
    )
    new_acc = run_acc * rescale[:, :, None] + product
    return (new_max, new_sum, new_acc)


def keep_totals(totals_in):
    return totals_in


def make_folder(segments, gathered_gates):

    def fold_keys(state_all, key_piece, first_key):
        key_part, value_part = key_piece
        key_total = key_part.shape[0]
        block_len = min(512, key_total)
        heads_dev = segments[0][0].shape[1]
        key_part = key_part.reshape(key_total, heads_dev, HD)
        value_part = value_part.reshape(key_total, heads_dev, HD)

        def one_block(block_index, state_now):
            offset = block_index * block_len
            key_rows = lax.dynamic_slice_in_dim(key_part, offset, block_len, 0)
            value_rows = lax.dynamic_slice_in_dim(value_part, offset, block_len, 0)
            key_pos = offset + jnp.arange(block_len, dtype=jnp.int32)
            key_gate = jnp.transpose(lax.dynamic_slice_in_dim(gathered_gates, offset, block_len, 0))
            updated = []
            for segment, totals_in in zip(segments, state_now):
                query_rows, query_gate, query_pos = segment
                needed = offset <= query_pos[-1]
                advance = partial(
                    attend_block,
                    query_rows=query_rows,
                    query_gate=query_gate,
                    query_pos=query_pos,
                    key_rows=key_rows,
                    value_rows=value_rows,
                    key_gate=key_gate,
                    key_pos=key_pos,
                )
                updated.append(lax.cond(needed, advance, keep_totals, totals_in))
            return tuple(updated)

        return lax.fori_loop(0, key_total // block_len, one_block, state_all)

    return fold_keys


MESH = pl.DeviceIdType.MESH
LANES = 128
QUADS = 4
LOG2E = 1.4426950408889634
PARTS = 2

TASKS = (
    ("zr", 1),
    ("fa", 0),
    ("zr", 2),
    ("fa", 1),
    ("s", 1),
    ("fa", 2),
    ("d", 0),
    ("s", 0),
    ("co1", 0),
    ("zr", 3),
    ("d", 1),
    ("s", 2),
    ("co1", 1),
    ("cp1", 1),
    ("d", 2),
    ("cp2", 1),
    ("fa", 3),
    ("co1", 2),
    ("co2", 1),
    ("r1", 1),
    ("cp1", 2),
    ("d", 3),
    ("cp2", 2),
    ("s", 3),
    ("r2", 1),
    ("co2", 2),
    ("r1", 2),
    ("cp1", 3),
    ("r3", 1),
    ("co1", 3),
    ("cp2", 3),
    ("r2", 2),
    ("co2", 0),
    ("co2", 3),
    ("r1", 3),
    ("r3", 2),
    ("cp1", 0),
    ("cp2", 0),
    ("r2", 3),
    ("r1", 0),
    ("r3", 3),
    ("r2", 0),
    ("r3", 0),
)


def layer_kernel(
    depth,
    queries_hbm,
    keys_hbm,
    values_hbm,
    gates_hbm,
    gain_hbm,
    stream_hbm,
    out_hbm,
    norm_hbm,
    routing_hbm,
    route_hbm,
    gate_hbm,
    up_hbm,
    down_hbm,
    out_ref,
    queries,
    stream,
    gain,
    norm_gain,
    routing,
    route_w,
    key_all,
    value_all,
    gate_all,
    weights_all,
    wcols,
    qcol,
    peak,
    weight_total,
    weighted,
    leaving,
    incoming,
    resid,
    out_w,
    rows_all,
    gate_w,
    up_w,
    down_w,
    hidden,
    mine,
    theirs,
    from_core,
    from_second,
    from_first,
    from_z,
    from_zf,
    local_sems,
    kv_send_sems,
    kv_recv_sems,
    out_send_sems,
    out_recv_sems,
    w_send_sems,
    w_recv_sems,
    wq_recv_sems,
    ag_send_sems,
    ag_recv_sems,
    rs_send_sems,
    core_sems,
    second_sems,
    first_sems,
    z_sems,
    zf_sems,
):
    sp = lax.axis_index("sp")
    tp = lax.axis_index("tp")
    tp_count = 2 * depth
    tokens = queries.shape[0]
    heads = queries.shape[1] // HD
    count, width = resid.shape
    units = gate_w.shape[1]
    part_rows = count // PARTS
    z, core = tp // 2, tp % 2
    other = 1 - core
    x_next = sp + 1 - 2 * (sp % 2)
    y_next = (sp + 2) % 4
    first = x_next * (1 - core) + y_next * core
    second = y_next * (1 - core) + x_next * core
    far = 3 - sp
    to_core = (sp, z * 2 + other)
    to_first = (first, tp)
    to_second = (second, tp)

    def f32(value):
        return value.astype(jnp.float32)

    def bf16(value):
        return value.astype(jnp.bfloat16)

    def at_z(level):
        return (sp, level * 2 + core)

    orders = []
    for at in range(depth):
        order = [at]
        for step in range(1, depth):
            pair = (at + step, at - step) if 2 * at < depth else (at - step, at + step)
            order += [lev for lev in pair if 0 <= lev < depth]
        orders.append(order)
    levels = []
    for place in range(depth):
        total = 0
        for at in range(depth):
            apart = (z - at + depth) % depth
            total = total + orders[at][place] * (1 - (apart + depth - 1) // depth)
        levels.append(total)

    def adjacent(level):
        return (level - z) * (level - z) == 1

    loads = {}

    def load(name, src, dst):
        loads[name] = pltpu.make_async_copy(src, dst, local_sems.at[len(loads)])
        loads[name].start()

    def head_cols(head):
        return slice(head * HD, (head + 1) * HD)

    load("gates", gates_hbm, gate_all.at[sp])
    for head in range(heads):
        load(("keys", head), keys_hbm.at[:, head_cols(head)], key_all.at[sp, head])
        load(("values", head), values_hbm.at[:, head_cols(head)], value_all.at[sp, head])
    load("queries", queries_hbm, queries)
    load("routing", routing_hbm, routing)
    load("route", route_hbm, route_w)

    barrier = pltpu.get_barrier_semaphore()
    peers = [to_first, to_second]
    peers += [(sp, (tp + step) % tp_count) for step in range(1, tp_count)]
    for peer in peers:
        pl.semaphore_signal(barrier, inc=1, device_id=peer, device_id_type=MESH)
    pl.semaphore_wait(barrier, len(peers))

    sent = []

    def send(src, dst, send_sem, recv_sem, target, when=None):
        copy = pltpu.make_async_remote_copy(
            src_ref=src,
            dst_ref=dst,
            send_sem=send_sem,
            recv_sem=recv_sem,
            device_id=target,
            device_id_type=MESH,
        )
        if when is None:
            copy.start()
        else:
            pl.when(when)(copy.start)
        sent.append((copy, when))

    def landed(dst, sem):
        pltpu.make_async_remote_copy(
            src_ref=dst,
            dst_ref=dst,
            send_sem=kv_send_sems.at[0],
            recv_sem=sem,
            device_id=to_core,
            device_id_type=MESH,
        ).wait_recv()

    def kv_refs(quad, head):
        refs = [(key_all.at[quad, head], 2 * head), (value_all.at[quad, head], 2 * head + 1)]
        return refs if head else [(gate_all.at[quad], 2 * heads)] + refs

    kv_count = [0]

    def kv_send(quad, head, target):
        for ref, part in kv_refs(quad, head):
            send(ref, ref, kv_send_sems.at[kv_count[0]], kv_recv_sems.at[quad, part], target)
            kv_count[0] += 1

    def kv_landed(quad, head):
        for ref, part in kv_refs(quad, head):
            landed(ref, kv_recv_sems.at[quad, part])

    loads["gates"].wait()
    for head in range(heads):
        loads["keys", head].wait()
        loads["values", head].wait()
        kv_send(sp, head, to_first)
        if head == 0:
            kv_send(sp, head, to_second)
    load("stream", stream_hbm, stream)
    load("gain", gain_hbm, gain)
    load("norm", norm_hbm, norm_gain)
    for head in range(heads):
        load(("out", head), out_hbm.at[:, head], out_w.at[head])
    load("gate", gate_hbm.at[0], gate_w)
    load("up", up_hbm.at[0], up_w)
    load("down", down_hbm.at[0], down_w)

    for name in ("routing", "route", "queries"):
        loads[name].wait()
    own_weights = weights_all.at[sp, tp]
    own_weights[...] = jnp.zeros_like(own_weights)
    for expert in range(QUADS):
        row = 0.0
        for k in range(routing.shape[0]):
            row = row + jnp.where(
                routing[k : k + 1, :] == expert, route_w[k : k + 1, :], 0.0
            )
        own_weights[expert : expert + 1, :count] = row

    chunk = LANES
    for head in range(heads):
        for at in range(tokens // chunk):
            span = slice(at * chunk, (at + 1) * chunk)
            row = gate_all[sp, head : head + 1, span] * LOG2E
            qcol[head, span] = jnp.transpose(jnp.broadcast_to(row, (chunk, chunk)))[:, :1]

    def attend(quad, head, diagonal):
        cols = head_cols(head)

        def attend_chunk(j):
            rows = pl.ds(pl.multiple_of(j * chunk, chunk), chunk)
            scores = lax.dot_general(
                queries[rows, cols],
                key_all[quad, head],
                (((1,), (1,)), ((), ())),
                preferred_element_type=jnp.float32,
            )
            query_gate = qcol[head, rows]
            key_gate = gate_all[quad, head : head + 1, :] * LOG2E
            scores = scores * (HD ** (-0.5) * LOG2E) - key_gate
            if diagonal:
                row_id = lax.broadcasted_iota(jnp.int32, scores.shape, 0) + j * chunk
                col_id = lax.broadcasted_iota(jnp.int32, scores.shape, 1)
                scores = jnp.where(col_id <= row_id, scores, masked_score)
            new_peak = jnp.max(scores, axis=1, keepdims=True) + query_gate
            if not diagonal:
                old_peak = peak[head, rows]
                new_peak = jnp.maximum(old_peak, new_peak)
            lifted = jnp.exp2(scores + (query_gate - new_peak))
            added = jnp.sum(lifted, axis=1, keepdims=True)
            product = jnp.dot(
                lifted.astype(jnp.bfloat16),
                value_all[quad, head],
                preferred_element_type=jnp.float32,
            )
            if not diagonal:
                rescale = jnp.exp2(old_peak - new_peak)
                added = weight_total[head, rows] * rescale + added
                product = weighted[head, rows] * rescale + product
            peak[head, rows] = new_peak
            weight_total[head, rows] = added
            weighted[head, rows] = product

        pairs = 2 if tokens % (2 * chunk) == 0 else 1

        @pl.loop(0, tokens // (pairs * chunk))
        def _(j):
            for at in range(pairs):
                attend_chunk(j * pairs + at)

    def attend_earlier(quad, head):
        @pl.when(quad < sp)
        def _():
            attend(quad, head, False)

    def take_first(head):
        kv_landed(first, head)
        kv_send(first, head, to_second)
        if head + 1 < heads:
            kv_send(sp, head + 1, to_second)
        attend_earlier(first, head)

    def take_second(head):
        kv_landed(second, head)
        attend_earlier(second, head)

    out_count = [0]

    def finish(head):
        kv_landed(far, head)
        attend_earlier(far, head)

        @pl.loop(0, tp_count)
        def _(j):
            rows = pl.ds(pl.multiple_of(j * count, count), count)
            attended = weighted[head, rows] / weight_total[head, rows]
            square = jnp.mean(attended * attended, axis=1, keepdims=True)
            normed = attended * lax.rsqrt(square + 1e-06) * gain[0:1, head_cols(head)]
            leaving[head, j] = normed.astype(jnp.bfloat16)

        for level in reversed(levels):
            for side in (core, other):
                if level is z_level and side is core:
                    continue
                target = level * 2 + side
                send(
                    leaving.at[head, target],
                    incoming.at[head, tp],
                    out_send_sems.at[out_count[0]],
                    out_recv_sems.at[head, tp],
                    (sp, target),
                )
                out_count[0] += 1
        incoming[head, tp] = leaving[head, tp]

    z_level = levels[0]
    for head in range(heads):
        attend(sp, head, True)
    for step in range(1, tp_count):
        target = (tp + step) % tp_count
        ref = weights_all.at[sp, tp]
        send(ref, ref, w_send_sems.at[step], w_recv_sems.at[tp], (sp, target))
    loads["gain"].wait()
    take_first(0)
    take_second(0)
    for head in range(heads):
        if head + 1 < heads:
            take_first(head + 1)
        finish(head)
        if head + 1 < heads:
            take_second(head + 1)
    for step in range(1, tp_count):
        source = (tp + step) % tp_count
        landed(weights_all.at[sp, source], w_recv_sems.at[source])

    send(weights_all.at[sp], weights_all.at[sp], w_send_sems.at[0], wq_recv_sems.at[sp], to_first)
    send(
        weights_all.at[sp],
        weights_all.at[sp],
        w_send_sems.at[tp_count],
        wq_recv_sems.at[sp],
        to_second,
    )
    loads["stream"].wait()
    resid[...] = f32(stream[...])
    loads["norm"].wait()
    landed(weights_all.at[first], wq_recv_sems.at[first])
    send(
        weights_all.at[first],
        weights_all.at[first],
        w_send_sems.at[tp_count + 1],
        wq_recv_sems.at[first],
        to_second,
    )
    strip = 512 if width % 512 == 0 else width
    for head in range(heads):
        loads["out", head].wait()
        for level in levels:
            sources = (level * 2, level * 2 + 1)
            for side in (core, other):
                source = level * 2 + side
                if not (level is z_level and side is core):
                    landed(incoming.at[head, source], out_recv_sems.at[head, source])

            @pl.loop(0, width // strip)
            def _(j, head=head, level=level, sources=sources):
                cols = pl.ds(pl.multiple_of(j * strip, strip), strip)
                rows = jnp.concatenate([incoming[head, source] for source in sources], axis=1)
                weights = out_w[head, pl.ds(level * 2, 2), :, cols].reshape(2 * HD, strip)
                resid[:, cols] += jnp.dot(rows, weights, preferred_element_type=jnp.float32)

    total = resid[...]
    center = total - jnp.mean(total, axis=1, keepdims=True)
    variance = jnp.mean(center * center, axis=1, keepdims=True)
    rows_all[core, z, sp] = (center * lax.rsqrt(variance + 1e-05) * norm_gain[0:1, :]).astype(
        jnp.bfloat16
    )

    ag_count = [0]

    def part_of(k):
        return pl.ds(k * part_rows, part_rows)

    def spread(level, quad, k, target, when=None):
        ref = rows_all.at[core, level, quad, part_of(k)]
        sem = ag_recv_sems.at[core, level, quad, k]
        send(ref, ref, ag_send_sems.at[ag_count[0]], sem, target, when)
        ag_count[0] += 1

    def arrived(half, level, quad, k):
        ref = rows_all.at[half, level, quad, part_of(k)]
        landed(ref, ag_recv_sems.at[half, level, quad, k])

    above, below = at_z((z + 1) % depth), at_z((z + depth - 1) % depth)
    for k in range(PARTS):
        spread(z, sp, k, above, z < depth - 1)
        spread(z, sp, k, below, z > 0)
        for target in (to_first, to_second, to_core):
            spread(z, sp, k, target)

    landed(weights_all.at[second], wq_recv_sems.at[second])
    landed(weights_all.at[far], wq_recv_sems.at[far])
    lane = lax.broadcasted_iota(jnp.int32, (QUADS, LANES), 0)
    picked = []
    for quad in range(QUADS):
        for source in range(tp_count):
            tile = weights_all[quad, source]
            picked.append(jnp.sum(jnp.where(lane == sp, tile, 0.0), axis=0, keepdims=True))
    fill = jnp.zeros((LANES - len(picked), LANES), jnp.float32)
    turned = jnp.transpose(jnp.concatenate(picked + [fill], axis=0))
    for quad in range(QUADS):
        for source in range(tp_count):
            at = quad * tp_count + source
            wcols[source % 2, source // 2, quad] = turned[:count, at : at + 1]

    for name in ("gate", "up", "down"):
        loads[name].wait()

    def hidden_units(half, level):
        piece = 512 if units % 512 == 0 else units

        @pl.loop(0, units // piece)
        def _(j):
            cols = pl.ds(pl.multiple_of(j * piece, piece), piece)
            block = rows_all[half, level].reshape(QUADS * count, width)
            gate_pre = jnp.dot(block, gate_w[:, cols], preferred_element_type=jnp.float32)
            up_pre = jnp.dot(block, up_w[:, cols], preferred_element_type=jnp.float32)
            hidden[half, level, :, cols] = bf16(gate_pre / (1.0 + jnp.exp(-gate_pre)) * up_pre)

    def down_product(half, level, dest):
        piece = 1024 if width % 1024 == 0 else width

        @pl.loop(0, width // piece)
        def _(j):
            cols = pl.ds(pl.multiple_of(j * piece, piece), piece)
            weight = wcols[half, level].reshape(QUADS * count, 1)
            product = jnp.dot(hidden[half, level], down_w[:, cols], preferred_element_type=jnp.float32)
            dest[level, :, :, cols] = bf16(product * weight).reshape(QUADS, count, piece)

    rs_count = [0]

    def send_back(src, dst, sem, target, when=None):
        send(src, dst, rs_send_sems.at[rs_count[0]], sem, target, when)
        rs_count[0] += 1

    def from_z_near(place):
        level = levels[place]
        for k in range(PARTS):
            arrived(core, level, sp, k)
            spread(level, sp, k, above, (level < z) & (z < depth - 1))
            spread(level, sp, k, below, (level > z) & (z > 0))
            spread(level, sp, k, to_first, (level - z) * (level - z) != 1)
            spread(level, sp, k, to_second)
            spread(level, sp, k, to_core)

    def from_first_near(place):
        level = levels[place]
        for k in range(PARTS):
            arrived(core, level, first, k)
            if place == 0:
                spread(level, first, k, above, z < depth - 1)
                spread(level, first, k, below, z > 0)
            spread(level, first, k, to_second)
            spread(level, first, k, to_core)

    def from_second_near(place):
        for k in range(PARTS):
            arrived(core, levels[place], second, k)
            spread(levels[place], second, k, to_core)

    def from_far(place):
        for k in range(PARTS):
            arrived(core, levels[place], far, k)
            spread(levels[place], far, k, to_core)

    def own_hidden(place):
        hidden_units(core, levels[place])

    def own_product(place):
        down_product(core, levels[place], mine)

    def partner_hidden(place):
        level = levels[place]
        for quad in range(QUADS):
            for k in range(PARTS):
                arrived(other, level, quad, k)
        hidden_units(other, level)

    def partner_product(place):
        level = levels[place]
        down_product(other, level, theirs)
        send_back(theirs.at[level], from_core.at[level], core_sems.at[level], to_core)

    def both_halves(place):
        level = levels[place]
        landed(from_core.at[level], core_sems.at[level])
        for slot, quad in ((1, far), (0, second)):
            for k in range(PARTS):
                rows = part_of(k)
                mine[level, quad, rows] = bf16(
                    f32(mine[level, quad, rows]) + f32(from_core[level, quad, rows])
                )
                send_back(
                    mine.at[level, quad, rows],
                    from_second.at[level, slot, rows],
                    second_sems.at[level, slot, k],
                    to_second,
                )

    def onto_first(place):
        level = levels[place]
        if place == 0:
            for near in levels[1:]:

                @pl.when(adjacent(near))
                def _(near=near):
                    for k in range(PARTS):
                        rows = part_of(k)
                        landed(from_zf.at[near, rows], zf_sems.at[near, k])
                    mine[z, first] = bf16(f32(mine[z, first]) + f32(from_zf[near]))

        for k in range(PARTS):
            rows = part_of(k)
            landed(from_second.at[level, 1, rows], second_sems.at[level, 1, k])
            mine[level, first, rows] = bf16(
                f32(mine[level, first, rows])
                + f32(from_core[level, first, rows])
                + f32(from_second[level, 1, rows])
            )
            src = mine.at[level, first, rows]
            dst, sem = from_first.at[level, rows], first_sems.at[level, k]
            if place:
                near = adjacent(level)
                send_back(src, from_zf.at[z, rows], zf_sems.at[z, k], at_z(level), near)
                send_back(src, dst, sem, to_first, (level - z) * (level - z) != 1)
            else:
                send_back(src, dst, sem, to_first)

    def onto_owner(place):
        level = levels[place]
        for k in range(PARTS):
            rows = part_of(k)
            landed(from_second.at[level, 0, rows], second_sems.at[level, 0, k])

            def total_of(with_first, rows=rows):
                total = f32(mine[level, sp, rows]) + f32(from_core[level, sp, rows])
                total = total + f32(from_second[level, 0, rows])
                return total + f32(from_first[level, rows]) if with_first else total

            if place == 0:
                landed(from_first.at[level, rows], first_sems.at[level, k])
                resid[rows] += total_of(True)
                continue

            @pl.when((level - z) * (level - z) != 1)
            def _(k=k, rows=rows, total_of=total_of):
                landed(from_first.at[level, rows], first_sems.at[level, k])
                mine[level, sp, rows] = bf16(total_of(True))

            @pl.when(adjacent(level))
            def _(rows=rows, total_of=total_of):
                mine[level, sp, rows] = bf16(total_of(False))

            src = mine.at[level, sp, rows]
            send_back(src, from_z.at[z, rows], z_sems.at[z, k], at_z(level))

    tasks = dict(
        zr=from_z_near,
        fa=from_first_near,
        s=from_second_near,
        d=from_far,
        co1=own_hidden,
        co2=own_product,
        cp1=partner_hidden,
        cp2=partner_product,
        r1=both_halves,
        r2=onto_first,
        r3=onto_owner,
    )
    for name, place in TASKS:
        tasks[name](place)

    total = resid[...]
    for near in levels[1:]:
        for k in range(PARTS):
            landed(from_z.at[near, part_of(k)], z_sems.at[near, k])
        total = total + f32(from_z[near])
    out_ref[...] = total.astype(out_ref.dtype)
    for copy, when in sent:
        if when is None:
            copy.wait_send()
        else:
            pl.when(when)(copy.wait_send)


def whole_layer(
    queries,
    keys,
    values,
    forget_totals,
    head_gain,
    stream,
    out_weight,
    norm_gain,
    routing,
    route_weights,
    gate_weight,
    up_weight,
    down_weight,
):
    tokens, wide = queries.shape
    heads = wide // HD
    count, width = stream.shape
    units = gate_weight.shape[2]
    tp_count = lax.axis_size("tp")
    depth = tp_count // 2
    top = routing.shape[1]
    bf16, f32 = jnp.bfloat16, jnp.float32
    dma = pltpu.SemaphoreType.DMA
    vmem = pltpu.VMEM
    plane = (depth, QUADS, count, width)
    hbm = pl.BlockSpec(memory_space=pltpu.HBM)
    ag_sends = PARTS * (5 + 5 * (depth - 1) + 2 * depth + 2 + 2 * depth)
    rs_sends = depth + PARTS * (2 * depth + 2 * depth + depth)
    return pl.pallas_call(
        partial(layer_kernel, depth),
        out_shape=jax.ShapeDtypeStruct((count, width), bf16),
        in_specs=[hbm] * 13,
        out_specs=pl.BlockSpec(memory_space=pltpu.VMEM),
        scratch_shapes=[
            vmem((tokens, wide), bf16),
            vmem((count, width), bf16),
            vmem((1, wide), f32),
            vmem((1, width), f32),
            vmem((top, count), jnp.int32),
            vmem((top, count), f32),
            vmem((QUADS, heads, tokens, HD), bf16),
            vmem((QUADS, heads, tokens, HD), bf16),
            vmem((QUADS, heads, tokens), f32),
            vmem((QUADS, tp_count, QUADS, LANES), f32),
            vmem((2, depth, QUADS, count, 1), f32),
            vmem((heads, tokens, 1), f32),
            vmem((heads, tokens, 1), f32),
            vmem((heads, tokens, 1), f32),
            vmem((heads, tokens, HD), f32),
            vmem((heads, tp_count, count, HD), bf16),
            vmem((heads, tp_count, count, HD), bf16),
            vmem((count, width), f32),
            vmem((heads, tp_count, HD, width), bf16),
            vmem((2,) + plane, bf16),
            vmem((width, units), bf16),
            vmem((width, units), bf16),
            vmem((units, width), bf16),
            vmem((2, depth, QUADS * count, units), bf16),
            vmem(plane, bf16),
            vmem(plane, bf16),
            vmem(plane, bf16),
            vmem((depth, 2, count, width), bf16),
            vmem((depth, count, width), bf16),
            vmem((depth, count, width), bf16),
            vmem((depth, count, width), bf16),
            dma((10 + 3 * heads,)),
            dma((3 + 6 * heads,)),
            dma((QUADS, 1 + 2 * heads)),
            dma((heads * (tp_count - 1),)),
            dma((heads, tp_count)),
            dma((tp_count + 2,)),
            dma((tp_count,)),
            dma((QUADS,)),
            dma((ag_sends,)),
            dma((2, depth, QUADS, PARTS)),
            dma((rs_sends,)),
            dma((depth,)),
            dma((depth, 2, PARTS)),
            dma((depth, PARTS)),
            dma((depth, PARTS)),
            dma((depth, PARTS)),
        ],
        compiler_params=pltpu.CompilerParams(
            collective_id=0, has_side_effects=True, vmem_limit_bytes=58 * 2**20
        ),
    )(
        queries,
        keys,
        values,
        jnp.transpose(forget_totals),
        head_gain.reshape(1, -1),
        stream,
        out_weight.reshape(tp_count, heads, HD, width),
        norm_gain.reshape(1, -1),
        jnp.transpose(routing),
        jnp.transpose(route_weights),
        gate_weight,
        up_weight,
        down_weight,
    )


def routed_experts(
    resid_sum, normed_rows, routing, route_weights, gate_weight, up_weight, down_weight
):
    sp_count = lax.axis_size("sp")
    row_count = normed_rows.shape[0]
    capacity = max(2, 2 * TOP * row_count // sp_count)
    flat_expert = routing.reshape(-1)
    onehot = (flat_expert[:, None] == jnp.arange(sp_count, dtype=jnp.int32)[None, :]).astype(
        jnp.int32
    )
    earlier = jnp.cumsum(onehot, axis=0) - onehot
    slot_index = flat_expert * capacity + jnp.sum(earlier * onehot, axis=1)
    slot_grid = slot_index.reshape(row_count, TOP)
    slot_ids = jnp.arange(sp_count * capacity, dtype=jnp.int32)
    placing = jnp.sum(
        (slot_grid[None, :, :] == slot_ids[:, None, None]).astype(jnp.float32), axis=2
    ).astype(jnp.bfloat16)
    outgoing = jnp.dot(placing, normed_rows, preferred_element_type=jnp.float32).astype(
        jnp.bfloat16
    )
    outgoing = outgoing.reshape(sp_count, capacity, normed_rows.shape[1])
    arrived = lax.all_to_all(outgoing, "sp", split_axis=0, concat_axis=0, tiled=True)
    row_piece = lax.all_gather(arrived.reshape(-1, arrived.shape[2]), "tp", axis=0, tiled=True)
    gate_pre = jnp.dot(row_piece, gate_weight[0], preferred_element_type=jnp.float32)
    up_pre = jnp.dot(row_piece, up_weight[0], preferred_element_type=jnp.float32)
    hidden = (jax.nn.silu(gate_pre) * up_pre).astype(jnp.bfloat16)
    summed = lax.psum_scatter(
        jnp.dot(hidden, down_weight[0], preferred_element_type=jnp.float32).astype(jnp.bfloat16),
        "tp",
        scatter_dimension=0,
        tiled=True,
    )
    expert_out = summed.reshape(sp_count, capacity, -1)
    returned = lax.all_to_all(expert_out, "sp", split_axis=0, concat_axis=0, tiled=True)
    picked = returned.reshape(sp_count * capacity, -1)[slot_index].astype(jnp.float32)
    weighted = picked * route_weights.reshape(-1)[:, None]
    routed = jnp.sum(weighted.reshape(row_count, TOP, -1), axis=1)
    return (resid_sum + routed).astype(jnp.bfloat16)


def on_device(
    queries,
    key_vectors,
    value_vectors,
    forget_totals,
    head_gain,
    stream,
    out_weight,
    norm_gain,
    routing,
    route_weights,
    gate_weight,
    up_weight,
    down_weight,
):
    rows_dev, sp_size, tp_size = stream.shape[0], lax.axis_size("sp"), lax.axis_size("tp")
    dense = 2 * TOP * rows_dev // sp_size >= rows_dev
    leveled = sp_size == QUADS and tp_size == 2 * len({place for _, place in TASKS})
    if dense and leveled and queries.shape[0] % LANES == 0 and rows_dev <= LANES and rows_dev % (16 * PARTS) == 0:
        return whole_layer(
            queries,
            key_vectors,
            value_vectors,
            forget_totals,
            head_gain,
            stream,
            out_weight,
            norm_gain,
            routing,
            route_weights,
            gate_weight,
            up_weight,
            down_weight,
        )
    tok_count = queries.shape[0]
    heads_dev = queries.shape[1] // HD
    sp_index = lax.axis_index("sp")
    sp_count = lax.axis_size("sp")
    gathered_gates = lax.all_gather(forget_totals, "sp", axis=0, tiled=True)
    first_pos = sp_index * tok_count
    query_pos = first_pos + jnp.arange(tok_count, dtype=jnp.int32)
    query_gate = jnp.transpose(lax.dynamic_slice_in_dim(gathered_gates, first_pos, tok_count, 0))
    segments = [(queries.reshape(tok_count, heads_dev, HD), query_gate, query_pos)]
    starting = (
        (
            jnp.full((heads_dev, tok_count), masked_score, jnp.float32),
            jnp.zeros((heads_dev, tok_count), jnp.float32),
            jnp.zeros((heads_dev, tok_count, HD), jnp.float32),
        ),
    )
    folder = make_folder(segments, gathered_gates)
    totals = folder(
        starting,
        (
            lax.all_gather(key_vectors, "sp", axis=0, tiled=True),
            lax.all_gather(value_vectors, "sp", axis=0, tiled=True),
        ),
        jnp.int32(0),
    )
    run_max, run_sum, run_acc = totals[0]
    attended = run_acc / run_sum[:, :, None]
    inverse_rms = lax.rsqrt(jnp.mean(attended * attended, axis=2, keepdims=True) + 1e-06)
    normed = attended * inverse_rms * head_gain.reshape(heads_dev, 1, HD)
    head_out = (
        jnp.transpose(normed, (1, 0, 2)).reshape(tok_count, heads_dev * HD).astype(jnp.bfloat16)
    )
    token_heads = lax.all_to_all(head_out, "tp", split_axis=0, concat_axis=1, tiled=True)
    mixed_rows = jnp.dot(token_heads, out_weight, preferred_element_type=jnp.float32)
    resid_sum = stream.astype(jnp.float32) + mixed_rows
    center = resid_sum - jnp.mean(resid_sum, axis=1, keepdims=True)
    normed_rows = (
        center * lax.rsqrt(jnp.mean(center * center, axis=1, keepdims=True) + 1e-05) * norm_gain
    ).astype(jnp.bfloat16)
    return routed_experts(
        resid_sum, normed_rows, routing, route_weights, gate_weight, up_weight, down_weight
    )


def solution(mesh):
    in_specs = (
        P("sp", "tp"),
        P("sp", "tp"),
        P("sp", "tp"),
        P("sp", "tp"),
        P("tp"),
        P(("sp", "tp"), None),
        P(),
        P(),
        P(("sp", "tp"), None),
        P(("sp", "tp"), None),
        P("sp", None, "tp"),
        P("sp", None, "tp"),
        P("sp", "tp", None),
    )
    out_specs = P(("sp", "tp"), None)
    return jax.shard_map(
        on_device, mesh=mesh, in_specs=in_specs, out_specs=out_specs, check_vma=False
    )
```

```python
from functools import partial

import jax
import jax.numpy as jnp
from jax import lax
from jax.experimental import pallas as pl
from jax.experimental.pallas import tpu as pltpu
from jax.sharding import PartitionSpec as P

HD = 128
TOP = 2


masked_score = -1e30


def attend_block(
    totals, query_rows, query_gate, query_pos, key_rows, value_rows, key_gate, key_pos
):
    run_max, run_sum, run_acc = totals
    scores = jnp.einsum("qhd,khd->hqk", query_rows, key_rows, preferred_element_type=jnp.float32)
    scores = scores * HD ** (-0.5) + query_gate[:, :, None] - key_gate[:, None, :]
    visible = (key_pos[None, :] <= query_pos[:, None])[None]
    scores = jnp.where(visible, scores, masked_score)
    new_max = jnp.maximum(run_max, jnp.max(scores, axis=2))
    lifted = jnp.where(visible, jnp.exp(scores - new_max[:, :, None]), 0.0)
    rescale = jnp.exp(run_max - new_max)
    new_sum = run_sum * rescale + jnp.sum(lifted, axis=2)
    product = jnp.einsum(
        "hqk,khd->hqd", lifted.astype(jnp.bfloat16), value_rows, preferred_element_type=jnp.float32
    )
    new_acc = run_acc * rescale[:, :, None] + product
    return (new_max, new_sum, new_acc)


def keep_totals(totals_in):
    return totals_in


def make_folder(segments, gathered_gates):

    def fold_keys(state_all, key_piece, first_key):
        key_part, value_part = key_piece
        key_total = key_part.shape[0]
        block_len = min(512, key_total)
        heads_dev = segments[0][0].shape[1]
        key_part = key_part.reshape(key_total, heads_dev, HD)
        value_part = value_part.reshape(key_total, heads_dev, HD)

        def one_block(block_index, state_now):
            offset = block_index * block_len
            key_rows = lax.dynamic_slice_in_dim(key_part, offset, block_len, 0)
            value_rows = lax.dynamic_slice_in_dim(value_part, offset, block_len, 0)
            key_pos = offset + jnp.arange(block_len, dtype=jnp.int32)
            key_gate = jnp.transpose(lax.dynamic_slice_in_dim(gathered_gates, offset, block_len, 0))
            updated = []
            for segment, totals_in in zip(segments, state_now):
                query_rows, query_gate, query_pos = segment
                needed = offset <= query_pos[-1]
                advance = partial(
                    attend_block,
                    query_rows=query_rows,
                    query_gate=query_gate,
                    query_pos=query_pos,
                    key_rows=key_rows,
                    value_rows=value_rows,
                    key_gate=key_gate,
                    key_pos=key_pos,
                )
                updated.append(lax.cond(needed, advance, keep_totals, totals_in))
            return tuple(updated)

        return lax.fori_loop(0, key_total // block_len, one_block, state_all)

    return fold_keys


MESH = pl.DeviceIdType.MESH
LANES = 128
QUADS = 4
LOG2E = 1.4426950408889634
PARTS = 2

TASKS = (
    ("zr", 1),
    ("fa", 0),
    ("zr", 2),
    ("fa", 1),
    ("s", 1),
    ("fa", 2),
    ("d", 0),
    ("s", 0),
    ("co1", 0),
    ("zr", 3),
    ("d", 1),
    ("s", 2),
    ("co1", 1),
    ("cp1", 1),
    ("d", 2),
    ("cp2", 1),
    ("fa", 3),
    ("co1", 2),
    ("co2", 1),
    ("r1", 1),
    ("cp1", 2),
    ("d", 3),
    ("cp2", 2),
    ("s", 3),
    ("r2", 1),
    ("co2", 2),
    ("r1", 2),
    ("cp1", 3),
    ("r3", 1),
    ("co1", 3),
    ("cp2", 3),
    ("r2", 2),
    ("co2", 0),
    ("co2", 3),
    ("r1", 3),
    ("r3", 2),
    ("cp1", 0),
    ("cp2", 0),
    ("r2", 3),
    ("r1", 0),
    ("r3", 3),
    ("r2", 0),
    ("r3", 0),
)


def layer_kernel(
    depth,
    queries_hbm,
    keys_hbm,
    values_hbm,
    gates_hbm,
    gain_hbm,
    stream_hbm,
    out_hbm,
    norm_hbm,
    routing_hbm,
    route_hbm,
    gate_hbm,
    up_hbm,
    down_hbm,
    out_ref,
    queries,
    stream,
    gain,
    norm_gain,
    routing,
    route_w,
    pair_all,
    gate_all,
    weights_all,
    wcols,
    qcol,
    peak,
    weight_total,
    weighted,
    leaving,
    incoming,
    resid,
    out_w,
    rows_all,
    gate_w,
    up_w,
    down_w,
    hidden,
    mine,
    theirs,
    from_core,
    from_second,
    from_first,
    from_z,
    from_zf,
    local_sems,
    kv_send_sems,
    kv_recv_sems,
    out_send_sems,
    out_recv_sems,
    w_send_sems,
    w_recv_sems,
    ag_send_sems,
    ag_recv_sems,
    part_recv_sems,
    rs_send_sems,
    core_sems,
    second_sems,
    first_sems,
    z_sems,
    zf_sems,
):
    sp = lax.axis_index("sp")
    tp = lax.axis_index("tp")
    tp_count = 2 * depth
    tokens = queries.shape[0]
    heads = queries.shape[1] // HD
    count, width = resid.shape
    units = gate_w.shape[1]
    part_rows = count // PARTS
    z, core = tp // 2, tp % 2
    other = 1 - core
    x_next = sp + 1 - 2 * (sp % 2)
    y_next = (sp + 2) % 4
    first = x_next * (1 - core) + y_next * core
    second = y_next * (1 - core) + x_next * core
    far = 3 - sp
    to_core = (sp, z * 2 + other)
    to_first = (first, tp)
    to_second = (second, tp)

    def f32(value):
        return value.astype(jnp.float32)

    def bf16(value):
        return value.astype(jnp.bfloat16)

    def at_z(level):
        return (sp, level * 2 + core)

    orders = []
    for at in range(depth):
        order = [at]
        for step in range(1, depth):
            pair = (at + step, at - step) if 2 * at < depth else (at - step, at + step)
            order += [lev for lev in pair if 0 <= lev < depth]
        orders.append(order)
    levels = []
    for place in range(depth):
        total = 0
        for at in range(depth):
            apart = (z - at + depth) % depth
            total = total + orders[at][place] * (1 - (apart + depth - 1) // depth)
        levels.append(total)

    def adjacent(level):
        return (level - z) * (level - z) == 1

    loads = {}

    def load(name, src, dst):
        loads[name] = pltpu.make_async_copy(src, dst, local_sems.at[len(loads)])
        loads[name].start()

    def head_cols(head):
        return slice(head * HD, (head + 1) * HD)

    load("gates", gates_hbm, gate_all.at[sp])
    for head in range(heads):
        load(("keys", head), keys_hbm.at[:, head_cols(head)], pair_all.at[sp, head, 0])
        load(("values", head), values_hbm.at[:, head_cols(head)], pair_all.at[sp, head, 1])
    load("queries", queries_hbm, queries)
    load("routing", routing_hbm, routing)
    load("route", route_hbm, route_w)

    barrier = pltpu.get_barrier_semaphore()
    peers = [to_first, to_second]
    peers += [(sp, (tp + step) % tp_count) for step in range(1, tp_count)]
    for peer in peers:
        pl.semaphore_signal(barrier, inc=1, device_id=peer, device_id_type=MESH)
    pl.semaphore_wait(barrier, len(peers))

    drains = []

    def send(src, dst, send_sem, recv_sem, target, when=None):
        copy = pltpu.make_async_remote_copy(
            src_ref=src,
            dst_ref=dst,
            send_sem=send_sem,
            recv_sem=recv_sem,
            device_id=target,
            device_id_type=MESH,
        )
        if when is None:
            copy.start()
        else:
            pl.when(when)(copy.start)

    def drain_later(ref, sem, when=None):
        drains.append((ref, sem, when))

    def landed(dst, sem):
        pltpu.make_async_remote_copy(
            src_ref=dst,
            dst_ref=dst,
            send_sem=kv_send_sems.at[0],
            recv_sem=sem,
            device_id=to_core,
            device_id_type=MESH,
        ).wait_recv()

    def kv_send(quad, head, target, lane):
        if head == 0:
            ref = gate_all.at[quad]
            send(ref, ref, kv_send_sems.at[2], kv_recv_sems.at[quad, heads], target)
        for ref in (pair_all.at[quad, head, 0], pair_all.at[quad, head, 1]):
            send(ref, ref, kv_send_sems.at[lane], kv_recv_sems.at[quad, head], target)

    def kv_landed(quad, head):
        if head == 0:
            landed(gate_all.at[quad], kv_recv_sems.at[quad, heads])
        landed(pair_all.at[quad, head], kv_recv_sems.at[quad, head])

    drain_later(pair_all.at[0], kv_send_sems.at[0])
    drain_later(pair_all.at[0:2], kv_send_sems.at[1])
    drain_later(gate_all.at[0:3], kv_send_sems.at[2])
    loads["gates"].wait()
    for head in range(heads):
        loads["keys", head].wait()
        loads["values", head].wait()
        kv_send(sp, head, to_first, 0)
        if head == 0:
            kv_send(sp, head, to_second, 1)
    load("stream", stream_hbm, stream)
    load("gain", gain_hbm, gain)
    load("norm", norm_hbm, norm_gain)
    for head in range(heads):
        load(("out", head), out_hbm.at[:, head], out_w.at[head])
    load("gate", gate_hbm.at[0], gate_w)
    load("up", up_hbm.at[0], up_w)
    load("down", down_hbm.at[0], down_w)

    for name in ("routing", "route", "queries"):
        loads[name].wait()
    own_weights = weights_all.at[sp, tp]
    own_weights[...] = jnp.zeros_like(own_weights)
    for expert in range(QUADS):
        row = 0.0
        for k in range(routing.shape[0]):
            row = row + jnp.where(
                routing[k : k + 1, :] == expert, route_w[k : k + 1, :], 0.0
            )
        own_weights[expert : expert + 1, :count] = row

    chunk = LANES
    for head in range(heads):
        for at in range(tokens // chunk):
            span = slice(at * chunk, (at + 1) * chunk)
            row = gate_all[sp, head : head + 1, span] * LOG2E
            qcol[head, span] = jnp.transpose(jnp.broadcast_to(row, (chunk, chunk)))[:, :1]

    def attend(quad, head, diagonal):
        cols = head_cols(head)

        def attend_chunk(j):
            rows = pl.ds(pl.multiple_of(j * chunk, chunk), chunk)
            scores = lax.dot_general(
                queries[rows, cols],
                pair_all[quad, head, 0],
                (((1,), (1,)), ((), ())),
                preferred_element_type=jnp.float32,
            )
            query_gate = qcol[head, rows]
            key_gate = gate_all[quad, head : head + 1, :] * LOG2E
            scores = scores * (HD ** (-0.5) * LOG2E) - key_gate
            if diagonal:
                row_id = lax.broadcasted_iota(jnp.int32, scores.shape, 0) + j * chunk
                col_id = lax.broadcasted_iota(jnp.int32, scores.shape, 1)
                scores = jnp.where(col_id <= row_id, scores, masked_score)
            new_peak = jnp.max(scores, axis=1, keepdims=True) + query_gate
            if not diagonal:
                old_peak = peak[head, rows]
                new_peak = jnp.maximum(old_peak, new_peak)
            lifted = jnp.exp2(scores + (query_gate - new_peak))
            added = jnp.sum(lifted, axis=1, keepdims=True)
            product = jnp.dot(
                lifted.astype(jnp.bfloat16),
                pair_all[quad, head, 1],
                preferred_element_type=jnp.float32,
            )
            if not diagonal:
                rescale = jnp.exp2(old_peak - new_peak)
                added = weight_total[head, rows] * rescale + added
                product = weighted[head, rows] * rescale + product
            peak[head, rows] = new_peak
            weight_total[head, rows] = added
            weighted[head, rows] = product

        pairs = 2 if tokens % (2 * chunk) == 0 else 1

        @pl.loop(0, tokens // (pairs * chunk))
        def _(j):
            for at in range(pairs):
                attend_chunk(j * pairs + at)

    def attend_earlier(quad, head):
        @pl.when(quad < sp)
        def _():
            attend(quad, head, False)

    def take_first(head):
        kv_landed(first, head)
        kv_send(first, head, to_second, 1)
        if head + 1 < heads:
            kv_send(sp, head + 1, to_second, 1)
        attend_earlier(first, head)

    def take_second(head):
        kv_landed(second, head)
        attend_earlier(second, head)

    def finish(head):
        kv_landed(far, head)
        attend_earlier(far, head)

        span = tokens // 2 if tp_count % 2 == 0 else tokens
        for at in range(tokens // span):
            rows = pl.ds(at * span, span)
            attended = weighted[head, rows] * (1.0 / weight_total[head, rows])
            square = jnp.mean(attended * attended, axis=1, keepdims=True)
            normed = attended * lax.rsqrt(square + 1e-06) * gain[0:1, head_cols(head)]
            blocks = span // count
            leaving[head, pl.ds(at * blocks, blocks)] = bf16(normed).reshape(blocks, count, HD)

        for level in reversed(levels):
            for side in (core, other):
                if level is z_level and side is core:
                    continue
                target = level * 2 + side
                send(
                    leaving.at[head, target],
                    incoming.at[head, tp],
                    out_send_sems.at[head],
                    out_recv_sems.at[head, z],
                    (sp, target),
                )
        drain_later(leaving.at[head, 0 : tp_count - 1], out_send_sems.at[head])
        incoming[head, tp] = leaving[head, tp]

    z_level = levels[0]
    for head in range(heads):
        attend(sp, head, True)
    for step in range(1, tp_count):
        target = (tp + step) % tp_count
        ref = weights_all.at[sp, tp]
        send(ref, ref, w_send_sems.at[0], w_recv_sems.at[QUADS], (sp, target))
    drain_later(weights_all.at[0, 0 : tp_count - 1], w_send_sems.at[0])
    loads["gain"].wait()
    take_first(0)
    take_second(0)
    for head in range(heads):
        if head + 1 < heads:
            take_first(head + 1)
        finish(head)
        if head + 1 < heads:
            take_second(head + 1)
    landed(weights_all.at[sp, 0 : tp_count - 1], w_recv_sems.at[QUADS])

    def spread_weights(quad, target):
        ref = weights_all.at[quad]
        send(ref, ref, w_send_sems.at[1], w_recv_sems.at[quad], target)

    spread_weights(sp, to_first)
    spread_weights(sp, to_second)
    drain_later(weights_all.at[0:3], w_send_sems.at[1])
    loads["stream"].wait()
    resid[...] = f32(stream[...])
    loads["norm"].wait()
    strip = 1024 if width % 1024 == 0 else width
    for head in range(heads):
        loads["out", head].wait()
        for level in levels:
            sources = (level * 2, level * 2 + 1)
            from_level = incoming.at[head, pl.ds(level * 2, 2)]
            if level is z_level:
                from_level = incoming.at[head, level * 2 + other]
            landed(from_level, out_recv_sems.at[head, level])

            @pl.loop(0, width // strip)
            def _(j, head=head, level=level, sources=sources):
                cols = pl.ds(pl.multiple_of(j * strip, strip), strip)
                rows = jnp.concatenate([incoming[head, source] for source in sources], axis=1)
                weights = out_w[head, pl.ds(level * 2, 2), :, cols].reshape(2 * HD, strip)
                resid[:, cols] += jnp.dot(rows, weights, preferred_element_type=jnp.float32)

    landed(weights_all.at[first], w_recv_sems.at[first])
    spread_weights(first, to_second)
    total = resid[...]
    center = total - jnp.mean(total, axis=1, keepdims=True)
    variance = jnp.mean(center * center, axis=1, keepdims=True)
    rows_all[core, z, sp] = (center * lax.rsqrt(variance + 1e-05) * norm_gain[0:1, :]).astype(
        jnp.bfloat16
    )

    ag_count = [3]

    def part_of(k):
        return pl.ds(k * part_rows, part_rows)

    def spread(level, quad, k, target, sem, recv_sem=None):
        ref = rows_all.at[core, level, quad, part_of(k)]
        if recv_sem is None:
            recv_sem = ag_recv_sems.at[level, quad, k]
        send(ref, ref, ag_send_sems.at[sem], recv_sem, target)

    def spread_all(level, quad, target, sem):
        for k in range(PARTS):
            spread(level, quad, k, target, sem)

    def to_partner(level, quad, k):
        spread(level, quad, k, to_core, 0, part_recv_sems.at[level])

    def lane_when(when):
        sem = ag_count[0]
        ag_count[0] += 1
        drain_later(rows_all.at[0, 0, 0], ag_send_sems.at[sem], when)

        def spread_when(level, quad, k, target):
            @pl.when(when)
            def _():
                spread(level, quad, k, target, sem)

        return spread_when

    def arrived(level, quad, k):
        landed(rows_all.at[core, level, quad, part_of(k)], ag_recv_sems.at[level, quad, k])

    drain_later(rows_all.at[0], ag_send_sems.at[0])
    drain_later(rows_all.at[0, 0:2], ag_send_sems.at[1])
    drain_later(rows_all.at[0, 0, 0], ag_send_sems.at[2])
    above, below = at_z((z + 1) % depth), at_z((z + depth - 1) % depth)
    own_above, own_below = lane_when(z < depth - 1), lane_when(z > 0)
    for k in range(PARTS):
        own_above(z, sp, k, above)
        own_below(z, sp, k, below)
        spread(z, sp, k, to_first, 2)
        spread(z, sp, k, to_second, 1)
        to_partner(z, sp, k)

    landed(weights_all.at[second], w_recv_sems.at[second])
    landed(weights_all.at[far], w_recv_sems.at[far])
    lane = lax.broadcasted_iota(jnp.int32, (QUADS, LANES), 0)
    picked = []
    for quad in range(QUADS):
        for source in range(tp_count):
            tile = weights_all[quad, source]
            picked.append(jnp.sum(jnp.where(lane == sp, tile, 0.0), axis=0, keepdims=True))
    fill = jnp.zeros((LANES - len(picked), LANES), jnp.float32)
    turned = jnp.transpose(jnp.concatenate(picked + [fill], axis=0))
    for quad in range(QUADS):
        for source in range(tp_count):
            at = quad * tp_count + source
            wcols[source % 2, source // 2, quad] = turned[:count, at : at + 1]

    for name in ("gate", "up", "down"):
        loads[name].wait()

    def hidden_units(half, level):
        piece = 512 if units % 512 == 0 else units

        @pl.loop(0, units // piece)
        def _(j):
            cols = pl.ds(pl.multiple_of(j * piece, piece), piece)
            block = rows_all[half, level].reshape(QUADS * count, width)
            gate_pre = jnp.dot(block, gate_w[:, cols], preferred_element_type=jnp.float32)
            up_pre = jnp.dot(block, up_w[:, cols], preferred_element_type=jnp.float32)
            hidden[half, level, :, cols] = bf16(gate_pre / (1.0 + jnp.exp(-gate_pre)) * up_pre)

    def down_product(half, level, dest):
        piece = 1024 if width % 1024 == 0 else width

        @pl.loop(0, width // piece)
        def _(j):
            cols = pl.ds(pl.multiple_of(j * piece, piece), piece)
            weight = wcols[half, level].reshape(QUADS * count, 1)
            product = jnp.dot(hidden[half, level], down_w[:, cols], preferred_element_type=jnp.float32)
            dest[level, :, :, cols] = bf16(product * weight).reshape(QUADS, count, piece)

    def from_z_near(place):
        level = levels[place]
        go_above = lane_when((level < z) & (z < depth - 1))
        go_below = lane_when((level > z) & (z > 0))
        go_first = lane_when((level - z) * (level - z) != 1)
        for k in range(PARTS):
            arrived(level, sp, k)
            go_above(level, sp, k, above)
            go_below(level, sp, k, below)
            go_first(level, sp, k, to_first)
            spread(level, sp, k, to_second, 1)
            to_partner(level, sp, k)

    def from_first_near(place):
        level = levels[place]
        if place == 0:
            go_above, go_below = lane_when(z < depth - 1), lane_when(z > 0)
        for k in range(PARTS):
            arrived(level, first, k)
            if place == 0:
                go_above(level, first, k, above)
                go_below(level, first, k, below)
            spread(level, first, k, to_second, 1)
            to_partner(level, first, k)

    def from_second_near(place):
        for k in range(PARTS):
            arrived(levels[place], second, k)
            to_partner(levels[place], second, k)

    def from_far(place):
        for k in range(PARTS):
            arrived(levels[place], far, k)
            to_partner(levels[place], far, k)

    def send_back(src, dst, lane, sem, target, when=None):
        send(src, dst, rs_send_sems.at[lane], sem, target, when)

    drain_later(mine, rs_send_sems.at[0])
    drain_later(rows_all.at[0, 0:2], rs_send_sems.at[1])
    drain_later(rows_all.at[0, 0, 0:3], rs_send_sems.at[2])
    drain_later(rows_all.at[0, 0, 0], rs_send_sems.at[3])

    def own_hidden(place):
        hidden_units(core, levels[place])

    def own_product(place):
        down_product(core, levels[place], mine)

    def partner_hidden(place):
        level = levels[place]
        landed(rows_all.at[other, level], part_recv_sems.at[level])
        hidden_units(other, level)

    def partner_product(place):
        level = levels[place]
        down_product(other, level, theirs)
        send_back(theirs.at[level], from_core.at[level], 0, core_sems.at[level], to_core)

    def both_halves(place):
        level = levels[place]
        landed(from_core.at[level], core_sems.at[level])
        for slot, quad in ((1, far), (0, second)):
            for k in range(PARTS):
                rows = part_of(k)
                mine[level, quad, rows] = bf16(
                    f32(mine[level, quad, rows]) + f32(from_core[level, quad, rows])
                )
                send_back(
                    mine.at[level, quad, rows],
                    from_second.at[level, slot, rows],
                    1,
                    second_sems.at[level, slot, k],
                    to_second,
                )

    def onto_first(place):
        level = levels[place]
        if place == 0:
            for near in levels[1:]:

                @pl.when(adjacent(near))
                def _(near=near):
                    for k in range(PARTS):
                        rows = part_of(k)
                        landed(from_zf.at[near, rows], zf_sems.at[near, k])
                    mine[z, first] = bf16(f32(mine[z, first]) + f32(from_zf[near]))

        near, apart = adjacent(level), (level - z) * (level - z) != 1
        if place:
            drain_later(rows_all.at[0, 0, 0], rs_send_sems.at[2 + 2 * place], near)
            drain_later(rows_all.at[0, 0, 0], rs_send_sems.at[3 + 2 * place], apart)
        for k in range(PARTS):
            rows = part_of(k)
            landed(from_second.at[level, 1, rows], second_sems.at[level, 1, k])
            mine[level, first, rows] = bf16(
                f32(mine[level, first, rows])
                + f32(from_core[level, first, rows])
                + f32(from_second[level, 1, rows])
            )
            src = mine.at[level, first, rows]
            dst, sem = from_first.at[level, rows], first_sems.at[level, k]
            if place:
                zf_dst, zf_sem = from_zf.at[z, rows], zf_sems.at[z, k]
                send_back(src, zf_dst, 2 + 2 * place, zf_sem, at_z(level), near)
                send_back(src, dst, 3 + 2 * place, sem, to_first, apart)
            else:
                send_back(src, dst, 3, sem, to_first)

    def onto_owner(place):
        level = levels[place]
        for k in range(PARTS):
            rows = part_of(k)
            landed(from_second.at[level, 0, rows], second_sems.at[level, 0, k])

            def total_of(with_first, rows=rows):
                total = f32(mine[level, sp, rows]) + f32(from_core[level, sp, rows])
                total = total + f32(from_second[level, 0, rows])
                return total + f32(from_first[level, rows]) if with_first else total

            if place == 0:
                landed(from_first.at[level, rows], first_sems.at[level, k])
                resid[rows] += total_of(True)
                continue

            @pl.when((level - z) * (level - z) != 1)
            def _(k=k, rows=rows, total_of=total_of):
                landed(from_first.at[level, rows], first_sems.at[level, k])
                mine[level, sp, rows] = bf16(total_of(True))

            @pl.when(adjacent(level))
            def _(rows=rows, total_of=total_of):
                mine[level, sp, rows] = bf16(total_of(False))

            src = mine.at[level, sp, rows]
            send_back(src, from_z.at[z, rows], 2, z_sems.at[z, k], at_z(level))

    tasks = dict(
        zr=from_z_near,
        fa=from_first_near,
        s=from_second_near,
        d=from_far,
        co1=own_hidden,
        co2=own_product,
        cp1=partner_hidden,
        cp2=partner_product,
        r1=both_halves,
        r2=onto_first,
        r3=onto_owner,
    )
    for name, place in TASKS:
        tasks[name](place)

    total = resid[...]
    for near in levels[1:]:
        for k in range(PARTS):
            landed(from_z.at[near, part_of(k)], z_sems.at[near, k])
        total = total + f32(from_z[near])
    out_ref[...] = total.astype(out_ref.dtype)

    def drain(ref, sem):
        pltpu.make_async_remote_copy(
            src_ref=ref,
            dst_ref=ref,
            send_sem=sem,
            recv_sem=kv_recv_sems.at[0, 0],
            device_id=to_core,
            device_id_type=MESH,
        ).wait_send()

    for ref, sem, when in drains:
        if when is None:
            drain(ref, sem)
        else:
            pl.when(when)(partial(drain, ref, sem))


def whole_layer(
    queries,
    keys,
    values,
    forget_totals,
    head_gain,
    stream,
    out_weight,
    norm_gain,
    routing,
    route_weights,
    gate_weight,
    up_weight,
    down_weight,
):
    tokens, wide = queries.shape
    heads = wide // HD
    count, width = stream.shape
    units = gate_weight.shape[2]
    tp_count = lax.axis_size("tp")
    depth = tp_count // 2
    top = routing.shape[1]
    bf16, f32 = jnp.bfloat16, jnp.float32
    dma = pltpu.SemaphoreType.DMA
    vmem = pltpu.VMEM
    plane = (depth, QUADS, count, width)
    hbm = pl.BlockSpec(memory_space=pltpu.HBM)
    return pl.pallas_call(
        partial(layer_kernel, depth),
        out_shape=jax.ShapeDtypeStruct((count, width), bf16),
        in_specs=[hbm] * 13,
        out_specs=pl.BlockSpec(memory_space=pltpu.VMEM),
        scratch_shapes=[
            vmem((tokens, wide), bf16),
            vmem((count, width), bf16),
            vmem((1, wide), f32),
            vmem((1, width), f32),
            vmem((top, count), jnp.int32),
            vmem((top, count), f32),
            vmem((QUADS, heads, 2, tokens, HD), bf16),
            vmem((QUADS, heads, tokens), f32),
            vmem((QUADS, tp_count, QUADS, LANES), f32),
            vmem((2, depth, QUADS, count, 1), f32),
            vmem((heads, tokens, 1), f32),
            vmem((heads, tokens, 1), f32),
            vmem((heads, tokens, 1), f32),
            vmem((heads, tokens, HD), f32),
            vmem((heads, tp_count, count, HD), bf16),
            vmem((heads, tp_count, count, HD), bf16),
            vmem((count, width), f32),
            vmem((heads, tp_count, HD, width), bf16),
            vmem((2,) + plane, bf16),
            vmem((width, units), bf16),
            vmem((width, units), bf16),
            vmem((units, width), bf16),
            vmem((2, depth, QUADS * count, units), bf16),
            vmem(plane, bf16),
            vmem(plane, bf16),
            vmem(plane, bf16),
            vmem((depth, 2, count, width), bf16),
            vmem((depth, count, width), bf16),
            vmem((depth, count, width), bf16),
            vmem((depth, count, width), bf16),
            dma((10 + 3 * heads,)),
            dma((3,)),
            dma((QUADS, heads + 1)),
            dma((heads,)),
            dma((heads, depth)),
            dma((2,)),
            dma((QUADS + 1,)),
            dma((3 + 2 + 2 + 3 * (depth - 1),)),
            dma((depth, QUADS, PARTS)),
            dma((depth,)),
            dma((2 + 2 * depth,)),
            dma((depth,)),
            dma((depth, 2, PARTS)),
            dma((depth, PARTS)),
            dma((depth, PARTS)),
            dma((depth, PARTS)),
        ],
        compiler_params=pltpu.CompilerParams(
            collective_id=0, has_side_effects=True, vmem_limit_bytes=50 * 2**20
        ),
    )(
        *(
            pltpu.with_memory_space_constraint(operand, pltpu.HBM)
            for operand in (
                queries,
                keys,
                values,
                jnp.transpose(forget_totals),
                head_gain.reshape(1, -1),
                stream,
                out_weight.reshape(tp_count, heads, HD, width),
                norm_gain.reshape(1, -1),
                jnp.transpose(routing),
                jnp.transpose(route_weights),
                gate_weight,
                up_weight,
                down_weight,
            )
        )
    )


def routed_experts(
    resid_sum, normed_rows, routing, route_weights, gate_weight, up_weight, down_weight
):
    sp_count = lax.axis_size("sp")
    row_count = normed_rows.shape[0]
    capacity = max(2, 2 * TOP * row_count // sp_count)
    flat_expert = routing.reshape(-1)
    onehot = (flat_expert[:, None] == jnp.arange(sp_count, dtype=jnp.int32)[None, :]).astype(
        jnp.int32
    )
    earlier = jnp.cumsum(onehot, axis=0) - onehot
    slot_index = flat_expert * capacity + jnp.sum(earlier * onehot, axis=1)
    slot_grid = slot_index.reshape(row_count, TOP)
    slot_ids = jnp.arange(sp_count * capacity, dtype=jnp.int32)
    placing = jnp.sum(
        (slot_grid[None, :, :] == slot_ids[:, None, None]).astype(jnp.float32), axis=2
    ).astype(jnp.bfloat16)
    outgoing = jnp.dot(placing, normed_rows, preferred_element_type=jnp.float32).astype(
        jnp.bfloat16
    )
    outgoing = outgoing.reshape(sp_count, capacity, normed_rows.shape[1])
    arrived = lax.all_to_all(outgoing, "sp", split_axis=0, concat_axis=0, tiled=True)
    row_piece = lax.all_gather(arrived.reshape(-1, arrived.shape[2]), "tp", axis=0, tiled=True)
    gate_pre = jnp.dot(row_piece, gate_weight[0], preferred_element_type=jnp.float32)
    up_pre = jnp.dot(row_piece, up_weight[0], preferred_element_type=jnp.float32)
    hidden = (jax.nn.silu(gate_pre) * up_pre).astype(jnp.bfloat16)
    summed = lax.psum_scatter(
        jnp.dot(hidden, down_weight[0], preferred_element_type=jnp.float32).astype(jnp.bfloat16),
        "tp",
        scatter_dimension=0,
        tiled=True,
    )
    expert_out = summed.reshape(sp_count, capacity, -1)
    returned = lax.all_to_all(expert_out, "sp", split_axis=0, concat_axis=0, tiled=True)
    picked = returned.reshape(sp_count * capacity, -1)[slot_index].astype(jnp.float32)
    weighted = picked * route_weights.reshape(-1)[:, None]
    routed = jnp.sum(weighted.reshape(row_count, TOP, -1), axis=1)
    return (resid_sum + routed).astype(jnp.bfloat16)


def on_device(
    queries,
    key_vectors,
    value_vectors,
    forget_totals,
    head_gain,
    stream,
    out_weight,
    norm_gain,
    routing,
    route_weights,
    gate_weight,
    up_weight,
    down_weight,
):
    rows_dev, sp_size, tp_size = stream.shape[0], lax.axis_size("sp"), lax.axis_size("tp")
    dense = 2 * TOP * rows_dev // sp_size >= rows_dev
    leveled = sp_size == QUADS and tp_size == 2 * len({place for _, place in TASKS})
    if dense and leveled and queries.shape[0] % LANES == 0 and rows_dev <= LANES and rows_dev % (16 * PARTS) == 0:
        return whole_layer(
            queries,
            key_vectors,
            value_vectors,
            forget_totals,
            head_gain,
            stream,
            out_weight,
            norm_gain,
            routing,
            route_weights,
            gate_weight,
            up_weight,
            down_weight,
        )
    tok_count = queries.shape[0]
    heads_dev = queries.shape[1] // HD
    sp_index = lax.axis_index("sp")
    sp_count = lax.axis_size("sp")
    gathered_gates = lax.all_gather(forget_totals, "sp", axis=0, tiled=True)
    first_pos = sp_index * tok_count
    query_pos = first_pos + jnp.arange(tok_count, dtype=jnp.int32)
    query_gate = jnp.transpose(lax.dynamic_slice_in_dim(gathered_gates, first_pos, tok_count, 0))
    segments = [(queries.reshape(tok_count, heads_dev, HD), query_gate, query_pos)]
    starting = (
        (
            jnp.full((heads_dev, tok_count), masked_score, jnp.float32),
            jnp.zeros((heads_dev, tok_count), jnp.float32),
            jnp.zeros((heads_dev, tok_count, HD), jnp.float32),
        ),
    )
    folder = make_folder(segments, gathered_gates)
    totals = folder(
        starting,
        (
            lax.all_gather(key_vectors, "sp", axis=0, tiled=True),
            lax.all_gather(value_vectors, "sp", axis=0, tiled=True),
        ),
        jnp.int32(0),
    )
    run_max, run_sum, run_acc = totals[0]
    attended = run_acc / run_sum[:, :, None]
    inverse_rms = lax.rsqrt(jnp.mean(attended * attended, axis=2, keepdims=True) + 1e-06)
    normed = attended * inverse_rms * head_gain.reshape(heads_dev, 1, HD)
    head_out = (
        jnp.transpose(normed, (1, 0, 2)).reshape(tok_count, heads_dev * HD).astype(jnp.bfloat16)
    )
    token_heads = lax.all_to_all(head_out, "tp", split_axis=0, concat_axis=1, tiled=True)
    mixed_rows = jnp.dot(token_heads, out_weight, preferred_element_type=jnp.float32)
    resid_sum = stream.astype(jnp.float32) + mixed_rows
    center = resid_sum - jnp.mean(resid_sum, axis=1, keepdims=True)
    normed_rows = (
        center * lax.rsqrt(jnp.mean(center * center, axis=1, keepdims=True) + 1e-05) * norm_gain
    ).astype(jnp.bfloat16)
    return routed_experts(
        resid_sum, normed_rows, routing, route_weights, gate_weight, up_weight, down_weight
    )


def solution(mesh):
    in_specs = (
        P("sp", "tp"),
        P("sp", "tp"),
        P("sp", "tp"),
        P("sp", "tp"),
        P("tp"),
        P(("sp", "tp"), None),
        P(),
        P(),
        P(("sp", "tp"), None),
        P(("sp", "tp"), None),
        P("sp", None, "tp"),
        P("sp", None, "tp"),
        P("sp", "tp", None),
    )
    out_specs = P(("sp", "tp"), None)
    return jax.shard_map(
        on_device, mesh=mesh, in_specs=in_specs, out_specs=out_specs, check_vma=False
    )
```

```python
from functools import partial

import jax
import jax.numpy as jnp
from jax import lax
from jax.experimental import pallas as pl
from jax.experimental.pallas import tpu as pltpu
from jax.sharding import PartitionSpec as P

HD = 128
TOP = 2


masked_score = -1e30


def attend_block(
    totals, query_rows, query_gate, query_pos, key_rows, value_rows, key_gate, key_pos
):
    run_max, run_sum, run_acc = totals
    scores = jnp.einsum("qhd,khd->hqk", query_rows, key_rows, preferred_element_type=jnp.float32)
    scores = scores * HD ** (-0.5) + query_gate[:, :, None] - key_gate[:, None, :]
    visible = (key_pos[None, :] <= query_pos[:, None])[None]
    scores = jnp.where(visible, scores, masked_score)
    new_max = jnp.maximum(run_max, jnp.max(scores, axis=2))
    lifted = jnp.where(visible, jnp.exp(scores - new_max[:, :, None]), 0.0)
    rescale = jnp.exp(run_max - new_max)
    new_sum = run_sum * rescale + jnp.sum(lifted, axis=2)
    product = jnp.einsum(
        "hqk,khd->hqd", lifted.astype(jnp.bfloat16), value_rows, preferred_element_type=jnp.float32
    )
    new_acc = run_acc * rescale[:, :, None] + product
    return (new_max, new_sum, new_acc)


def keep_totals(totals_in):
    return totals_in


def make_folder(segments, gathered_gates):

    def fold_keys(state_all, key_piece, first_key):
        key_part, value_part = key_piece
        key_total = key_part.shape[0]
        block_len = min(512, key_total)
        heads_dev = segments[0][0].shape[1]
        key_part = key_part.reshape(key_total, heads_dev, HD)
        value_part = value_part.reshape(key_total, heads_dev, HD)

        def one_block(block_index, state_now):
            offset = block_index * block_len
            key_rows = lax.dynamic_slice_in_dim(key_part, offset, block_len, 0)
            value_rows = lax.dynamic_slice_in_dim(value_part, offset, block_len, 0)
            key_pos = offset + jnp.arange(block_len, dtype=jnp.int32)
            key_gate = jnp.transpose(lax.dynamic_slice_in_dim(gathered_gates, offset, block_len, 0))
            updated = []
            for segment, totals_in in zip(segments, state_now):
                query_rows, query_gate, query_pos = segment
                needed = offset <= query_pos[-1]
                advance = partial(
                    attend_block,
                    query_rows=query_rows,
                    query_gate=query_gate,
                    query_pos=query_pos,
                    key_rows=key_rows,
                    value_rows=value_rows,
                    key_gate=key_gate,
                    key_pos=key_pos,
                )
                updated.append(lax.cond(needed, advance, keep_totals, totals_in))
            return tuple(updated)

        return lax.fori_loop(0, key_total // block_len, one_block, state_all)

    return fold_keys


MESH = pl.DeviceIdType.MESH
LANES = 128
QUADS = 4
LOG2E = 1.4426950408889634
PARTS = 2

TASKS = (
    ("zr", 1),
    ("fa", 0),
    ("zr", 2),
    ("fa", 1),
    ("s", 1),
    ("fa", 2),
    ("d", 0),
    ("s", 0),
    ("co1", 0),
    ("zr", 3),
    ("d", 1),
    ("s", 2),
    ("co1", 1),
    ("cp1", 1),
    ("d", 2),
    ("cp2", 1),
    ("fa", 3),
    ("co1", 2),
    ("co2", 1),
    ("r1", 1),
    ("cp1", 2),
    ("d", 3),
    ("cp2", 2),
    ("s", 3),
    ("r2", 1),
    ("co2", 2),
    ("r1", 2),
    ("cp1", 3),
    ("r3", 1),
    ("co1", 3),
    ("cp2", 3),
    ("r2", 2),
    ("co2", 0),
    ("co2", 3),
    ("r1", 3),
    ("r3", 2),
    ("cp1", 0),
    ("cp2", 0),
    ("r2", 3),
    ("r1", 0),
    ("r3", 3),
    ("r2", 0),
    ("r3", 0),
)


def layer_kernel(
    depth,
    queries_hbm,
    keys_hbm,
    values_hbm,
    gates_hbm,
    gain_hbm,
    stream_hbm,
    out_hbm,
    norm_hbm,
    routing_hbm,
    route_hbm,
    gate_hbm,
    up_hbm,
    down_hbm,
    out_ref,
    queries,
    stream,
    gain,
    norm_gain,
    routing,
    route_w,
    pair_all,
    gate_all,
    weights_all,
    wcols,
    qcol,
    peak,
    weight_total,
    weighted,
    leaving,
    incoming,
    resid,
    out_w,
    rows_all,
    gate_w,
    up_w,
    down_w,
    hidden,
    mine,
    theirs,
    from_core,
    from_second,
    from_first,
    from_z,
    from_zf,
    word_sems,
    local_sems,
    kv_send_sems,
    kv_recv_sems,
    out_send_sems,
    out_recv_sems,
    w_send_sems,
    w_recv_sems,
    ag_send_sems,
    ag_recv_sems,
    part_recv_sems,
    rs_send_sems,
    core_sems,
    second_sems,
    first_sems,
    z_sems,
    zf_sems,
):
    sp = lax.axis_index("sp")
    tp = lax.axis_index("tp")
    tp_count = 2 * depth
    tokens = queries.shape[0]
    heads = queries.shape[1] // HD
    count, width = resid.shape
    units = gate_w.shape[1]
    part_rows = count // PARTS
    z, core = tp // 2, tp % 2
    other = 1 - core
    x_next = sp + 1 - 2 * (sp % 2)
    y_next = (sp + 2) % 4
    first = x_next * (1 - core) + y_next * core
    second = y_next * (1 - core) + x_next * core
    far = 3 - sp
    to_core = (sp, z * 2 + other)
    to_first = (first, tp)
    to_second = (second, tp)

    def f32(value):
        return value.astype(jnp.float32)

    def bf16(value):
        return value.astype(jnp.bfloat16)

    def at_z(level):
        return (sp, level * 2 + core)

    orders = []
    for at in range(depth):
        order = [at]
        for step in range(1, depth):
            pair = (at + step, at - step) if 2 * at < depth else (at - step, at + step)
            order += [lev for lev in pair if 0 <= lev < depth]
        orders.append(order)
    levels = []
    for place in range(depth):
        total = 0
        for at in range(depth):
            apart = (z - at + depth) % depth
            total = total + orders[at][place] * (1 - (apart + depth - 1) // depth)
        levels.append(total)

    def adjacent(level):
        return (level - z) * (level - z) == 1

    loads = {}

    def load(name, src, dst):
        loads[name] = pltpu.make_async_copy(src, dst, local_sems.at[len(loads)])
        loads[name].start()

    def head_cols(head):
        return slice(head * HD, (head + 1) * HD)

    load("gates", gates_hbm, gate_all.at[sp])
    for head in range(heads):
        load(("keys", head), keys_hbm.at[:, head_cols(head)], pair_all.at[sp, head, 0])
        load(("values", head), values_hbm.at[:, head_cols(head)], pair_all.at[sp, head, 1])
    load("queries", queries_hbm, queries)
    load("routing", routing_hbm, routing)
    load("route", route_hbm, route_w)

    barrier = pltpu.get_barrier_semaphore()
    inner = z * (depth - 1 - z)
    above, below = at_z((z + 1) % depth), at_z((z + depth - 1) % depth)

    def greet(sems):
        sides = ((None, to_core, 0), (z < depth - 1, above, 1), (z > 0, below, 2))
        for when, peer, side in sides:

            def signal(peer=peer, side=side):
                pl.semaphore_signal(sems(side), inc=1, device_id=peer, device_id_type=MESH)

            if when is None:
                signal()
            else:
                pl.when(when)(signal)

    for peer in (to_first, to_second):
        pl.semaphore_signal(barrier, inc=1, device_id=peer, device_id_type=MESH)
    greet(lambda side: barrier)
    pl.semaphore_wait(barrier, 5 - 1 // (1 + inner))

    def word(stage):
        greet(lambda side: word_sems.at[stage, side])

    def hear(stage):
        for when, side in ((None, 0), (z > 0, 1), (z < depth - 1, 2)):

            def listen(side=side):
                pl.semaphore_wait(word_sems.at[stage, side], 1)

            if when is None:
                listen()
            else:
                pl.when(when)(listen)

    drains = []

    def send(src, dst, send_sem, recv_sem, target, when=None):
        copy = pltpu.make_async_remote_copy(
            src_ref=src,
            dst_ref=dst,
            send_sem=send_sem,
            recv_sem=recv_sem,
            device_id=target,
            device_id_type=MESH,
        )
        if when is None:
            copy.start()
        else:
            pl.when(when)(copy.start)

    def drain_later(ref, sem, when=None):
        drains.append((ref, sem, when))

    def landed(dst, sem):
        pltpu.make_async_remote_copy(
            src_ref=dst,
            dst_ref=dst,
            send_sem=kv_send_sems.at[0],
            recv_sem=sem,
            device_id=to_core,
            device_id_type=MESH,
        ).wait_recv()

    def kv_send(quad, head, target, lane):
        if head == 0:
            ref = gate_all.at[quad]
            send(ref, ref, kv_send_sems.at[2], kv_recv_sems.at[quad, heads], target)
        for ref in (pair_all.at[quad, head, 0], pair_all.at[quad, head, 1]):
            send(ref, ref, kv_send_sems.at[lane], kv_recv_sems.at[quad, head], target)

    def kv_landed(quad, head):
        if head == 0:
            landed(gate_all.at[quad], kv_recv_sems.at[quad, heads])
        landed(pair_all.at[quad, head], kv_recv_sems.at[quad, head])

    drain_later(pair_all.at[0], kv_send_sems.at[0])
    drain_later(pair_all.at[0:2], kv_send_sems.at[1])
    drain_later(gate_all.at[0:3], kv_send_sems.at[2])
    loads["gates"].wait()
    for head in range(heads):
        loads["keys", head].wait()
        loads["values", head].wait()
        kv_send(sp, head, to_first, 0)
        if head == 0:
            kv_send(sp, head, to_second, 1)
    load("stream", stream_hbm, stream)
    load("gain", gain_hbm, gain)
    load("norm", norm_hbm, norm_gain)
    for head in range(heads):
        load(("out", head), out_hbm.at[:, head], out_w.at[head])
    load("gate", gate_hbm.at[0], gate_w)
    load("up", up_hbm.at[0], up_w)
    load("down", down_hbm.at[0], down_w)

    for name in ("routing", "route", "queries"):
        loads[name].wait()
    own_weights = weights_all.at[sp, tp]
    own_weights[...] = jnp.zeros_like(own_weights)
    for expert in range(QUADS):
        row = 0.0
        for k in range(routing.shape[0]):
            row = row + jnp.where(
                routing[k : k + 1, :] == expert, route_w[k : k + 1, :], 0.0
            )
        own_weights[expert : expert + 1, :count] = row

    chunk = LANES
    for head in range(heads):
        for at in range(tokens // chunk):
            span = slice(at * chunk, (at + 1) * chunk)
            row = gate_all[sp, head : head + 1, span] * LOG2E
            qcol[head, span] = jnp.transpose(jnp.broadcast_to(row, (chunk, chunk)))[:, :1]

    halves = 2 if tokens % (2 * chunk) == 0 and tp_count % 2 == 0 else 1

    def attend(quad, head, diagonal, parts):
        cols = head_cols(head)

        def attend_chunk(j):
            start = j * chunk
            rows = pl.ds(start if isinstance(start, int) else pl.multiple_of(start, chunk), chunk)
            scores = lax.dot_general(
                queries[rows, cols],
                pair_all[quad, head, 0],
                (((1,), (1,)), ((), ())),
                preferred_element_type=jnp.float32,
            )
            query_gate = qcol[head, rows]
            key_gate = gate_all[quad, head : head + 1, :] * LOG2E
            scores = scores * (HD ** (-0.5) * LOG2E) - key_gate
            if diagonal:
                row_id = lax.broadcasted_iota(jnp.int32, scores.shape, 0) + start
                col_id = lax.broadcasted_iota(jnp.int32, scores.shape, 1)
                scores = jnp.where(col_id <= row_id, scores, masked_score)
            new_peak = jnp.max(scores, axis=1, keepdims=True) + query_gate
            if not diagonal:
                old_peak = peak[head, rows]
                new_peak = jnp.maximum(old_peak, new_peak)
            lifted = jnp.exp2(scores + (query_gate - new_peak))
            added = jnp.sum(lifted, axis=1, keepdims=True)
            product = jnp.dot(
                lifted.astype(jnp.bfloat16),
                pair_all[quad, head, 1],
                preferred_element_type=jnp.float32,
            )
            if not diagonal:
                rescale = jnp.exp2(old_peak - new_peak)
                added = weight_total[head, rows] * rescale + added
                product = weighted[head, rows] * rescale + product
            return rows, new_peak, added, product

        group = tokens // (halves * chunk)

        def attend_group(j):
            for rows, new_peak, added, product in [attend_chunk(j * group + at) for at in range(group)]:
                peak[head, rows] = new_peak
                weight_total[head, rows] = added
                weighted[head, rows] = product

        for part in parts:
            attend_group(part)

    def attend_earlier(quad, head, parts=tuple(range(halves))):
        @pl.when(quad < sp)
        def _():
            attend(quad, head, False, parts)

    def take_first(head):
        kv_landed(first, head)
        kv_send(first, head, to_second, 1)
        if head + 1 < heads:
            kv_send(sp, head + 1, to_second, 1)
        attend_earlier(first, head)

    def take_second(head):
        kv_landed(second, head)
        attend_earlier(second, head)

    def finish(head):
        kv_landed(far, head)
        span, blocks = tokens // halves, tp_count // halves
        for part in range(halves):
            attend_earlier(far, head, (part,))
            rows = pl.ds(part * span, span)
            attended = weighted[head, rows] * (1.0 / weight_total[head, rows])
            square = jnp.mean(attended * attended, axis=1, keepdims=True)
            normed = attended * lax.rsqrt(square + 1e-06) * gain[0:1, head_cols(head)]
            targets = range(part * blocks, (part + 1) * blocks)
            leaving[head, targets.start : targets.stop] = bf16(normed).reshape(blocks, count, HD)
            for target in targets:

                @pl.when(tp != target)
                def _(target=target):
                    send(
                        leaving.at[head, target],
                        incoming.at[head, tp],
                        out_send_sems.at[head],
                        out_recv_sems.at[head, z],
                        (sp, target),
                    )

        drain_later(leaving.at[head, 0 : tp_count - 1], out_send_sems.at[head])
        incoming[head, tp] = leaving[head, tp]

    z_level = levels[0]
    word(0)
    for head in range(heads):
        attend(sp, head, True, range(halves))
    for stage in range(depth - 1):
        hear(stage)
        if stage + 1 < depth - 1:
            word(stage + 1)
    for step in range(1, tp_count):
        target = (tp + step) % tp_count
        ref = weights_all.at[sp, tp]
        send(ref, ref, w_send_sems.at[0], w_recv_sems.at[QUADS], (sp, target))
    drain_later(weights_all.at[0, 0 : tp_count - 1], w_send_sems.at[0])
    loads["gain"].wait()
    take_first(0)
    take_second(0)
    for head in range(heads):
        if head + 1 < heads:
            take_first(head + 1)
        finish(head)
        if head + 1 < heads:
            take_second(head + 1)
    landed(weights_all.at[sp, 0 : tp_count - 1], w_recv_sems.at[QUADS])

    def spread_weights(quad, target):
        ref = weights_all.at[quad]
        send(ref, ref, w_send_sems.at[1], w_recv_sems.at[quad], target)

    spread_weights(sp, to_first)
    spread_weights(sp, to_second)
    drain_later(weights_all.at[0:3], w_send_sems.at[1])
    loads["stream"].wait()
    resid[...] = f32(stream[...])
    loads["norm"].wait()
    strip = 1024 if width % 1024 == 0 else width
    for head in range(heads):
        loads["out", head].wait()
        for level in levels:
            sources = (level * 2, level * 2 + 1)
            from_level = incoming.at[head, pl.ds(level * 2, 2)]
            if level is z_level:
                from_level = incoming.at[head, level * 2 + other]
            landed(from_level, out_recv_sems.at[head, level])

            @pl.loop(0, width // strip)
            def _(j, head=head, level=level, sources=sources):
                cols = pl.ds(pl.multiple_of(j * strip, strip), strip)
                rows = jnp.concatenate([incoming[head, source] for source in sources], axis=1)
                weights = out_w[head, pl.ds(level * 2, 2), :, cols].reshape(2 * HD, strip)
                resid[:, cols] += jnp.dot(rows, weights, preferred_element_type=jnp.float32)

    landed(weights_all.at[first], w_recv_sems.at[first])
    spread_weights(first, to_second)
    total = resid[...]
    center = total - jnp.mean(total, axis=1, keepdims=True)
    variance = jnp.mean(center * center, axis=1, keepdims=True)
    rows_all[core, z, sp] = (center * lax.rsqrt(variance + 1e-05) * norm_gain[0:1, :]).astype(
        jnp.bfloat16
    )

    ag_count = [3]

    def part_of(k):
        return pl.ds(k * part_rows, part_rows)

    def spread(level, quad, k, target, sem, recv_sem=None):
        ref = rows_all.at[core, level, quad, part_of(k)]
        if recv_sem is None:
            recv_sem = ag_recv_sems.at[level, quad, k]
        send(ref, ref, ag_send_sems.at[sem], recv_sem, target)

    def spread_all(level, quad, target, sem):
        for k in range(PARTS):
            spread(level, quad, k, target, sem)

    def to_partner(level, quad, k):
        spread(level, quad, k, to_core, 0, part_recv_sems.at[level])

    def lane_when(when):
        sem = ag_count[0]
        ag_count[0] += 1
        drain_later(rows_all.at[0, 0, 0], ag_send_sems.at[sem], when)

        def spread_when(level, quad, k, target):
            @pl.when(when)
            def _():
                spread(level, quad, k, target, sem)

        return spread_when

    def arrived(level, quad, k):
        landed(rows_all.at[core, level, quad, part_of(k)], ag_recv_sems.at[level, quad, k])

    drain_later(rows_all.at[0], ag_send_sems.at[0])
    drain_later(rows_all.at[0, 0:2], ag_send_sems.at[1])
    drain_later(rows_all.at[0, 0, 0], ag_send_sems.at[2])
    own_above, own_below = lane_when(z < depth - 1), lane_when(z > 0)
    for k in range(PARTS):
        own_above(z, sp, k, above)
        own_below(z, sp, k, below)
        spread(z, sp, k, to_first, 2)
        spread(z, sp, k, to_second, 1)
        to_partner(z, sp, k)

    landed(weights_all.at[second], w_recv_sems.at[second])
    landed(weights_all.at[far], w_recv_sems.at[far])
    lane = lax.broadcasted_iota(jnp.int32, (QUADS, LANES), 0)
    picked = []
    for quad in range(QUADS):
        for source in range(tp_count):
            tile = weights_all[quad, source]
            picked.append(jnp.sum(jnp.where(lane == sp, tile, 0.0), axis=0, keepdims=True))
    fill = jnp.zeros((LANES - len(picked), LANES), jnp.float32)
    turned = jnp.transpose(jnp.concatenate(picked + [fill], axis=0))
    for quad in range(QUADS):
        for source in range(tp_count):
            at = quad * tp_count + source
            wcols[source % 2, source // 2, quad] = turned[:count, at : at + 1]

    for name in ("gate", "up", "down"):
        loads[name].wait()

    def hidden_units(half, level):
        piece = 512 if units % 512 == 0 else units

        @pl.loop(0, units // piece)
        def _(j):
            cols = pl.ds(pl.multiple_of(j * piece, piece), piece)
            block = rows_all[half, level].reshape(QUADS * count, width)
            gate_pre = jnp.dot(block, gate_w[:, cols], preferred_element_type=jnp.float32)
            up_pre = jnp.dot(block, up_w[:, cols], preferred_element_type=jnp.float32)
            hidden[half, level, :, cols] = bf16(gate_pre / (1.0 + jnp.exp(-gate_pre)) * up_pre)

    def down_product(half, level, dest):
        piece = 1024 if width % 1024 == 0 else width

        @pl.loop(0, width // piece)
        def _(j):
            cols = pl.ds(pl.multiple_of(j * piece, piece), piece)
            weight = wcols[half, level].reshape(QUADS * count, 1)
            product = jnp.dot(hidden[half, level], down_w[:, cols], preferred_element_type=jnp.float32)
            dest[level, :, :, cols] = bf16(product * weight).reshape(QUADS, count, piece)

    def from_z_near(place):
        level = levels[place]
        go_above = lane_when((level < z) & (z < depth - 1))
        go_below = lane_when((level > z) & (z > 0))
        go_first = lane_when((level - z) * (level - z) != 1)
        for k in range(PARTS):
            arrived(level, sp, k)
            go_above(level, sp, k, above)
            go_below(level, sp, k, below)
            go_first(level, sp, k, to_first)
            spread(level, sp, k, to_second, 1)
            to_partner(level, sp, k)

    def from_first_near(place):
        level = levels[place]
        if place == 0:
            go_above, go_below = lane_when(z < depth - 1), lane_when(z > 0)
        for k in range(PARTS):
            arrived(level, first, k)
            if place == 0:
                go_above(level, first, k, above)
                go_below(level, first, k, below)
            spread(level, first, k, to_second, 1)
            to_partner(level, first, k)

    def from_second_near(place):
        for k in range(PARTS):
            arrived(levels[place], second, k)
            to_partner(levels[place], second, k)

    def from_far(place):
        for k in range(PARTS):
            arrived(levels[place], far, k)
            to_partner(levels[place], far, k)

    def send_back(src, dst, lane, sem, target, when=None):
        send(src, dst, rs_send_sems.at[lane], sem, target, when)

    drain_later(mine, rs_send_sems.at[0])
    drain_later(rows_all.at[0, 0:2], rs_send_sems.at[1])
    drain_later(rows_all.at[0, 0, 0:3], rs_send_sems.at[2])
    drain_later(rows_all.at[0, 0, 0], rs_send_sems.at[3])

    def own_hidden(place):
        hidden_units(core, levels[place])

    def own_product(place):
        down_product(core, levels[place], mine)

    def partner_hidden(place):
        level = levels[place]
        landed(rows_all.at[other, level], part_recv_sems.at[level])
        hidden_units(other, level)

    def partner_product(place):
        level = levels[place]
        down_product(other, level, theirs)
        send_back(theirs.at[level], from_core.at[level], 0, core_sems.at[level], to_core)

    def both_halves(place):
        level = levels[place]
        landed(from_core.at[level], core_sems.at[level])
        for slot, quad in ((1, far), (0, second)):
            for k in range(PARTS):
                rows = part_of(k)
                mine[level, quad, rows] = bf16(
                    f32(mine[level, quad, rows]) + f32(from_core[level, quad, rows])
                )
                send_back(
                    mine.at[level, quad, rows],
                    from_second.at[level, slot, rows],
                    1,
                    second_sems.at[level, slot, k],
                    to_second,
                )

    def onto_first(place):
        level = levels[place]
        if place == 0:
            for near in levels[1:]:

                @pl.when(adjacent(near))
                def _(near=near):
                    for k in range(PARTS):
                        rows = part_of(k)
                        landed(from_zf.at[near, rows], zf_sems.at[near, k])
                    mine[z, first] = bf16(f32(mine[z, first]) + f32(from_zf[near]))

        near, apart = adjacent(level), (level - z) * (level - z) != 1
        if place:
            drain_later(rows_all.at[0, 0, 0], rs_send_sems.at[2 + 2 * place], near)
            drain_later(rows_all.at[0, 0, 0], rs_send_sems.at[3 + 2 * place], apart)
        for k in range(PARTS):
            rows = part_of(k)
            landed(from_second.at[level, 1, rows], second_sems.at[level, 1, k])
            mine[level, first, rows] = bf16(
                f32(mine[level, first, rows])
                + f32(from_core[level, first, rows])
                + f32(from_second[level, 1, rows])
            )
            src = mine.at[level, first, rows]
            dst, sem = from_first.at[level, rows], first_sems.at[level, k]
            if place:
                zf_dst, zf_sem = from_zf.at[z, rows], zf_sems.at[z, k]
                send_back(src, zf_dst, 2 + 2 * place, zf_sem, at_z(level), near)
                send_back(src, dst, 3 + 2 * place, sem, to_first, apart)
            else:
                send_back(src, dst, 3, sem, to_first)

    def onto_owner(place):
        level = levels[place]
        for k in range(PARTS):
            rows = part_of(k)
            landed(from_second.at[level, 0, rows], second_sems.at[level, 0, k])

            def total_of(with_first, rows=rows):
                total = f32(mine[level, sp, rows]) + f32(from_core[level, sp, rows])
                total = total + f32(from_second[level, 0, rows])
                return total + f32(from_first[level, rows]) if with_first else total

            if place == 0:
                landed(from_first.at[level, rows], first_sems.at[level, k])
                resid[rows] += total_of(True)
                continue

            @pl.when((level - z) * (level - z) != 1)
            def _(k=k, rows=rows, total_of=total_of):
                landed(from_first.at[level, rows], first_sems.at[level, k])
                mine[level, sp, rows] = bf16(total_of(True))

            @pl.when(adjacent(level))
            def _(rows=rows, total_of=total_of):
                mine[level, sp, rows] = bf16(total_of(False))

            src = mine.at[level, sp, rows]
            send_back(src, from_z.at[z, rows], 2, z_sems.at[z, k], at_z(level))

    tasks = dict(
        zr=from_z_near,
        fa=from_first_near,
        s=from_second_near,
        d=from_far,
        co1=own_hidden,
        co2=own_product,
        cp1=partner_hidden,
        cp2=partner_product,
        r1=both_halves,
        r2=onto_first,
        r3=onto_owner,
    )
    for name, place in TASKS:
        tasks[name](place)

    total = resid[...]
    for near in levels[1:]:
        for k in range(PARTS):
            landed(from_z.at[near, part_of(k)], z_sems.at[near, k])
        total = total + f32(from_z[near])
    out_ref[...] = total.astype(out_ref.dtype)

    def drain(ref, sem):
        pltpu.make_async_remote_copy(
            src_ref=ref,
            dst_ref=ref,
            send_sem=sem,
            recv_sem=kv_recv_sems.at[0, 0],
            device_id=to_core,
            device_id_type=MESH,
        ).wait_send()

    for ref, sem, when in drains:
        if when is None:
            drain(ref, sem)
        else:
            pl.when(when)(partial(drain, ref, sem))


def whole_layer(
    queries,
    keys,
    values,
    forget_totals,
    head_gain,
    stream,
    out_weight,
    norm_gain,
    routing,
    route_weights,
    gate_weight,
    up_weight,
    down_weight,
):
    tokens, wide = queries.shape
    heads = wide // HD
    count, width = stream.shape
    units = gate_weight.shape[2]
    tp_count = lax.axis_size("tp")
    depth = tp_count // 2
    top = routing.shape[1]
    bf16, f32 = jnp.bfloat16, jnp.float32
    dma = pltpu.SemaphoreType.DMA
    vmem = pltpu.VMEM
    plane = (depth, QUADS, count, width)
    hbm = pl.BlockSpec(memory_space=pltpu.HBM)
    return pl.pallas_call(
        partial(layer_kernel, depth),
        out_shape=jax.ShapeDtypeStruct((count, width), bf16),
        in_specs=[hbm] * 13,
        out_specs=pl.BlockSpec(memory_space=pltpu.VMEM),
        scratch_shapes=[
            vmem((tokens, wide), bf16),
            vmem((count, width), bf16),
            vmem((1, wide), f32),
            vmem((1, width), f32),
            vmem((top, count), jnp.int32),
            vmem((top, count), f32),
            vmem((QUADS, heads, 2, tokens, HD), bf16),
            vmem((QUADS, heads, tokens), f32),
            vmem((QUADS, tp_count, QUADS, LANES), f32),
            vmem((2, depth, QUADS, count, 1), f32),
            vmem((heads, tokens, 1), f32),
            vmem((heads, tokens, 1), f32),
            vmem((heads, tokens, 1), f32),
            vmem((heads, tokens, HD), f32),
            vmem((heads, tp_count, count, HD), bf16),
            vmem((heads, tp_count, count, HD), bf16),
            vmem((count, width), f32),
            vmem((heads, tp_count, HD, width), bf16),
            vmem((2,) + plane, bf16),
            vmem((width, units), bf16),
            vmem((width, units), bf16),
            vmem((units, width), bf16),
            vmem((2, depth, QUADS * count, units), bf16),
            vmem(plane, bf16),
            vmem(plane, bf16),
            vmem(plane, bf16),
            vmem((depth, 2, count, width), bf16),
            vmem((depth, count, width), bf16),
            vmem((depth, count, width), bf16),
            vmem((depth, count, width), bf16),
            pltpu.SemaphoreType.REGULAR((depth - 1, 3)),
            dma((10 + 3 * heads,)),
            dma((3,)),
            dma((QUADS, heads + 1)),
            dma((heads,)),
            dma((heads, depth)),
            dma((2,)),
            dma((QUADS + 1,)),
            dma((3 + 2 + 2 + 3 * (depth - 1),)),
            dma((depth, QUADS, PARTS)),
            dma((depth,)),
            dma((2 + 2 * depth,)),
            dma((depth,)),
            dma((depth, 2, PARTS)),
            dma((depth, PARTS)),
            dma((depth, PARTS)),
            dma((depth, PARTS)),
        ],
        compiler_params=pltpu.CompilerParams(
            collective_id=0, has_side_effects=True, vmem_limit_bytes=50 * 2**20
        ),
    )(
        *(
            pltpu.with_memory_space_constraint(operand, pltpu.HBM)
            for operand in (
                queries,
                keys,
                values,
                jnp.transpose(forget_totals),
                head_gain.reshape(1, -1),
                stream,
                out_weight.reshape(tp_count, heads, HD, width),
                norm_gain.reshape(1, -1),
                jnp.transpose(routing),
                jnp.transpose(route_weights),
                gate_weight,
                up_weight,
                down_weight,
            )
        )
    )


def routed_experts(
    resid_sum, normed_rows, routing, route_weights, gate_weight, up_weight, down_weight
):
    sp_count = lax.axis_size("sp")
    row_count = normed_rows.shape[0]
    capacity = max(2, 2 * TOP * row_count // sp_count)
    flat_expert = routing.reshape(-1)
    onehot = (flat_expert[:, None] == jnp.arange(sp_count, dtype=jnp.int32)[None, :]).astype(
        jnp.int32
    )
    earlier = jnp.cumsum(onehot, axis=0) - onehot
    slot_index = flat_expert * capacity + jnp.sum(earlier * onehot, axis=1)
    slot_grid = slot_index.reshape(row_count, TOP)
    slot_ids = jnp.arange(sp_count * capacity, dtype=jnp.int32)
    placing = jnp.sum(
        (slot_grid[None, :, :] == slot_ids[:, None, None]).astype(jnp.float32), axis=2
    ).astype(jnp.bfloat16)
    outgoing = jnp.dot(placing, normed_rows, preferred_element_type=jnp.float32).astype(
        jnp.bfloat16
    )
    outgoing = outgoing.reshape(sp_count, capacity, normed_rows.shape[1])
    arrived = lax.all_to_all(outgoing, "sp", split_axis=0, concat_axis=0, tiled=True)
    row_piece = lax.all_gather(arrived.reshape(-1, arrived.shape[2]), "tp", axis=0, tiled=True)
    gate_pre = jnp.dot(row_piece, gate_weight[0], preferred_element_type=jnp.float32)
    up_pre = jnp.dot(row_piece, up_weight[0], preferred_element_type=jnp.float32)
    hidden = (jax.nn.silu(gate_pre) * up_pre).astype(jnp.bfloat16)
    summed = lax.psum_scatter(
        jnp.dot(hidden, down_weight[0], preferred_element_type=jnp.float32).astype(jnp.bfloat16),
        "tp",
        scatter_dimension=0,
        tiled=True,
    )
    expert_out = summed.reshape(sp_count, capacity, -1)
    returned = lax.all_to_all(expert_out, "sp", split_axis=0, concat_axis=0, tiled=True)
    picked = returned.reshape(sp_count * capacity, -1)[slot_index].astype(jnp.float32)
    weighted = picked * route_weights.reshape(-1)[:, None]
    routed = jnp.sum(weighted.reshape(row_count, TOP, -1), axis=1)
    return (resid_sum + routed).astype(jnp.bfloat16)


def on_device(
    queries,
    key_vectors,
    value_vectors,
    forget_totals,
    head_gain,
    stream,
    out_weight,
    norm_gain,
    routing,
    route_weights,
    gate_weight,
    up_weight,
    down_weight,
):
    rows_dev, sp_size, tp_size = stream.shape[0], lax.axis_size("sp"), lax.axis_size("tp")
    dense = 2 * TOP * rows_dev // sp_size >= rows_dev
    leveled = sp_size == QUADS and tp_size == 2 * len({place for _, place in TASKS})
    if dense and leveled and queries.shape[0] % LANES == 0 and rows_dev <= LANES and rows_dev % (16 * PARTS) == 0:
        return whole_layer(
            queries,
            key_vectors,
            value_vectors,
            forget_totals,
            head_gain,
            stream,
            out_weight,
            norm_gain,
            routing,
            route_weights,
            gate_weight,
            up_weight,
            down_weight,
        )
    tok_count = queries.shape[0]
    heads_dev = queries.shape[1] // HD
    sp_index = lax.axis_index("sp")
    sp_count = lax.axis_size("sp")
    gathered_gates = lax.all_gather(forget_totals, "sp", axis=0, tiled=True)
    first_pos = sp_index * tok_count
    query_pos = first_pos + jnp.arange(tok_count, dtype=jnp.int32)
    query_gate = jnp.transpose(lax.dynamic_slice_in_dim(gathered_gates, first_pos, tok_count, 0))
    segments = [(queries.reshape(tok_count, heads_dev, HD), query_gate, query_pos)]
    starting = (
        (
            jnp.full((heads_dev, tok_count), masked_score, jnp.float32),
            jnp.zeros((heads_dev, tok_count), jnp.float32),
            jnp.zeros((heads_dev, tok_count, HD), jnp.float32),
        ),
    )
    folder = make_folder(segments, gathered_gates)
    totals = folder(
        starting,
        (
            lax.all_gather(key_vectors, "sp", axis=0, tiled=True),
            lax.all_gather(value_vectors, "sp", axis=0, tiled=True),
        ),
        jnp.int32(0),
    )
    run_max, run_sum, run_acc = totals[0]
    attended = run_acc / run_sum[:, :, None]
    inverse_rms = lax.rsqrt(jnp.mean(attended * attended, axis=2, keepdims=True) + 1e-06)
    normed = attended * inverse_rms * head_gain.reshape(heads_dev, 1, HD)
    head_out = (
        jnp.transpose(normed, (1, 0, 2)).reshape(tok_count, heads_dev * HD).astype(jnp.bfloat16)
    )
    token_heads = lax.all_to_all(head_out, "tp", split_axis=0, concat_axis=1, tiled=True)
    mixed_rows = jnp.dot(token_heads, out_weight, preferred_element_type=jnp.float32)
    resid_sum = stream.astype(jnp.float32) + mixed_rows
    center = resid_sum - jnp.mean(resid_sum, axis=1, keepdims=True)
    normed_rows = (
        center * lax.rsqrt(jnp.mean(center * center, axis=1, keepdims=True) + 1e-05) * norm_gain
    ).astype(jnp.bfloat16)
    return routed_experts(
        resid_sum, normed_rows, routing, route_weights, gate_weight, up_weight, down_weight
    )


def solution(mesh):
    in_specs = (
        P("sp", "tp"),
        P("sp", "tp"),
        P("sp", "tp"),
        P("sp", "tp"),
        P("tp"),
        P(("sp", "tp"), None),
        P(),
        P(),
        P(("sp", "tp"), None),
        P(("sp", "tp"), None),
        P("sp", None, "tp"),
        P("sp", None, "tp"),
        P("sp", "tp", None),
    )
    out_specs = P(("sp", "tp"), None)
    return jax.shard_map(
        on_device, mesh=mesh, in_specs=in_specs, out_specs=out_specs, check_vma=False
    )
```

```python
from functools import partial

import jax
import jax.numpy as jnp
from jax import lax
from jax.experimental import pallas as pl
from jax.experimental.pallas import tpu as pltpu
from jax.sharding import PartitionSpec as P

HD = 128
TOP = 2


masked_score = -1e30


def attend_block(
    totals, query_rows, query_gate, query_pos, key_rows, value_rows, key_gate, key_pos
):
    run_max, run_sum, run_acc = totals
    scores = jnp.einsum("qhd,khd->hqk", query_rows, key_rows, preferred_element_type=jnp.float32)
    scores = scores * HD ** (-0.5) + query_gate[:, :, None] - key_gate[:, None, :]
    visible = (key_pos[None, :] <= query_pos[:, None])[None]
    scores = jnp.where(visible, scores, masked_score)
    new_max = jnp.maximum(run_max, jnp.max(scores, axis=2))
    lifted = jnp.where(visible, jnp.exp(scores - new_max[:, :, None]), 0.0)
    rescale = jnp.exp(run_max - new_max)
    new_sum = run_sum * rescale + jnp.sum(lifted, axis=2)
    product = jnp.einsum(
        "hqk,khd->hqd", lifted.astype(jnp.bfloat16), value_rows, preferred_element_type=jnp.float32
    )
    new_acc = run_acc * rescale[:, :, None] + product
    return (new_max, new_sum, new_acc)


def keep_totals(totals_in):
    return totals_in


def make_folder(segments, gathered_gates):

    def fold_keys(state_all, key_piece, first_key):
        key_part, value_part = key_piece
        key_total = key_part.shape[0]
        block_len = min(512, key_total)
        heads_dev = segments[0][0].shape[1]
        key_part = key_part.reshape(key_total, heads_dev, HD)
        value_part = value_part.reshape(key_total, heads_dev, HD)

        def one_block(block_index, state_now):
            offset = block_index * block_len
            key_rows = lax.dynamic_slice_in_dim(key_part, offset, block_len, 0)
            value_rows = lax.dynamic_slice_in_dim(value_part, offset, block_len, 0)
            key_pos = offset + jnp.arange(block_len, dtype=jnp.int32)
            key_gate = jnp.transpose(lax.dynamic_slice_in_dim(gathered_gates, offset, block_len, 0))
            updated = []
            for segment, totals_in in zip(segments, state_now):
                query_rows, query_gate, query_pos = segment
                needed = offset <= query_pos[-1]
                advance = partial(
                    attend_block,
                    query_rows=query_rows,
                    query_gate=query_gate,
                    query_pos=query_pos,
                    key_rows=key_rows,
                    value_rows=value_rows,
                    key_gate=key_gate,
                    key_pos=key_pos,
                )
                updated.append(lax.cond(needed, advance, keep_totals, totals_in))
            return tuple(updated)

        return lax.fori_loop(0, key_total // block_len, one_block, state_all)

    return fold_keys


MESH = pl.DeviceIdType.MESH
LANES = 128
QUADS = 4
LOG2E = 1.4426950408889634
PARTS = 2

TASKS = (
    ("zr", 1),
    ("fa", 0),
    ("s", 1),
    ("zr", 2),
    ("fa", 1),
    ("fa", 2),
    ("zr", 3),
    ("d", 1),
    ("co1", 1),
    ("cp1", 1),
    ("d", 2),
    ("cp2", 1),
    ("s", 2),
    ("fa", 3),
    ("co1", 2),
    ("co2", 1),
    ("r1", 1),
    ("s", 3),
    ("cp1", 2),
    ("cp2", 2),
    ("r2", 1),
    ("d", 3),
    ("co2", 2),
    ("r1", 2),
    ("cp1", 3),
    ("r3", 1),
    ("d", 0),
    ("cp2", 3),
    ("s", 0),
    ("r2", 2),
    ("co1", 3),
    ("co2", 3),
    ("r1", 3),
    ("r3", 2),
    ("cp1", 0),
    ("cp2", 0),
    ("r2", 3),
    ("co1", 0),
    ("co2", 0),
    ("r1", 0),
    ("r3", 3),
    ("r2", 0),
    ("r3", 0),
)


def layer_kernel(
    depth,
    queries_hbm,
    keys_hbm,
    values_hbm,
    gates_hbm,
    gain_hbm,
    stream_hbm,
    out_hbm,
    norm_hbm,
    routing_hbm,
    route_hbm,
    gate_hbm,
    up_hbm,
    down_hbm,
    out_ref,
    queries,
    stream,
    gain,
    norm_gain,
    routing,
    route_w,
    pair_all,
    gate_all,
    weights_all,
    wcols,
    qcol,
    peak,
    weight_total,
    weighted,
    leaving,
    incoming,
    resid,
    out_w,
    rows_all,
    gate_w,
    up_w,
    down_w,
    hidden,
    mine,
    theirs,
    from_core,
    from_second,
    from_first,
    from_z,
    from_zf,
    word_sems,
    local_sems,
    kv_send_sems,
    kv_recv_sems,
    out_send_sems,
    out_recv_sems,
    w_send_sems,
    w_recv_sems,
    ag_send_sems,
    ag_recv_sems,
    part_recv_sems,
    rs_send_sems,
    core_sems,
    second_sems,
    first_sems,
    z_sems,
    zf_sems,
):
    sp = lax.axis_index("sp")
    tp = lax.axis_index("tp")
    tp_count = 2 * depth
    tokens = queries.shape[0]
    heads = queries.shape[1] // HD
    count, width = resid.shape
    units = gate_w.shape[1]
    part_rows = count // PARTS
    z, core = tp // 2, tp % 2
    other = 1 - core
    x_next = sp + 1 - 2 * (sp % 2)
    y_next = (sp + 2) % 4
    first = x_next * (1 - core) + y_next * core
    second = y_next * (1 - core) + x_next * core
    far = 3 - sp
    to_core = (sp, z * 2 + other)
    to_first = (first, tp)
    to_second = (second, tp)

    def f32(value):
        return value.astype(jnp.float32)

    def bf16(value):
        return value.astype(jnp.bfloat16)

    def at_z(level):
        return (sp, level * 2 + core)

    orders = []
    for at in range(depth):
        order = [at]
        for step in range(1, depth):
            pair = (at + step, at - step) if 2 * at < depth else (at - step, at + step)
            order += [lev for lev in pair if 0 <= lev < depth]
        orders.append(order)
    levels = []
    for place in range(depth):
        total = 0
        for at in range(depth):
            apart = (z - at + depth) % depth
            total = total + orders[at][place] * (1 - (apart + depth - 1) // depth)
        levels.append(total)

    def adjacent(level):
        return (level - z) * (level - z) == 1

    loads = {}

    def load(name, src, dst):
        loads[name] = pltpu.make_async_copy(src, dst, local_sems.at[len(loads)])
        loads[name].start()

    def head_cols(head):
        return slice(head * HD, (head + 1) * HD)

    load("gates", gates_hbm, gate_all.at[sp])
    for head in range(heads):
        load(("keys", head), keys_hbm.at[:, head_cols(head)], pair_all.at[sp, head, 0])
        load(("values", head), values_hbm.at[:, head_cols(head)], pair_all.at[sp, head, 1])
    load("queries", queries_hbm, queries)
    load("routing", routing_hbm, routing)
    load("route", route_hbm, route_w)

    barrier = pltpu.get_barrier_semaphore()
    inner = z * (depth - 1 - z)
    above, below = at_z((z + 1) % depth), at_z((z + depth - 1) % depth)

    def greet(sems):
        sides = ((None, to_core, 0), (z < depth - 1, above, 1), (z > 0, below, 2))
        for when, peer, side in sides:

            def signal(peer=peer, side=side):
                pl.semaphore_signal(sems(side), inc=1, device_id=peer, device_id_type=MESH)

            if when is None:
                signal()
            else:
                pl.when(when)(signal)

    for peer in (to_first, to_second):
        pl.semaphore_signal(barrier, inc=1, device_id=peer, device_id_type=MESH)
    greet(lambda side: barrier)
    pl.semaphore_wait(barrier, 5 - 1 // (1 + inner))

    def word(stage):
        greet(lambda side: word_sems.at[stage, side])

    def hear(stage):
        for when, side in ((None, 0), (z > 0, 1), (z < depth - 1, 2)):

            def listen(side=side):
                pl.semaphore_wait(word_sems.at[stage, side], 1)

            if when is None:
                listen()
            else:
                pl.when(when)(listen)

    drains = []

    def send(src, dst, send_sem, recv_sem, target, when=None):
        copy = pltpu.make_async_remote_copy(
            src_ref=src,
            dst_ref=dst,
            send_sem=send_sem,
            recv_sem=recv_sem,
            device_id=target,
            device_id_type=MESH,
        )
        if when is None:
            copy.start()
        else:
            pl.when(when)(copy.start)

    def drain_later(ref, sem, when=None):
        drains.append((ref, sem, when))

    def landed(dst, sem):
        pltpu.make_async_remote_copy(
            src_ref=dst,
            dst_ref=dst,
            send_sem=kv_send_sems.at[0],
            recv_sem=sem,
            device_id=to_core,
            device_id_type=MESH,
        ).wait_recv()

    def kv_send(quad, head, target, lane):
        if head == 0:
            ref = gate_all.at[quad]
            send(ref, ref, kv_send_sems.at[2], kv_recv_sems.at[quad, heads], target)
        for ref in (pair_all.at[quad, head, 0], pair_all.at[quad, head, 1]):
            send(ref, ref, kv_send_sems.at[lane], kv_recv_sems.at[quad, head], target)

    def kv_landed(quad, head):
        if head == 0:
            landed(gate_all.at[quad], kv_recv_sems.at[quad, heads])
        landed(pair_all.at[quad, head], kv_recv_sems.at[quad, head])

    drain_later(pair_all.at[0], kv_send_sems.at[0])
    drain_later(pair_all.at[0:2], kv_send_sems.at[1])
    drain_later(gate_all.at[0:3], kv_send_sems.at[2])
    loads["gates"].wait()
    for head in range(heads):
        loads["keys", head].wait()
        loads["values", head].wait()
        kv_send(sp, head, to_first, 0)
        if head == 0:
            kv_send(sp, head, to_second, 1)
    load("stream", stream_hbm, stream)
    load("gain", gain_hbm, gain)
    load("norm", norm_hbm, norm_gain)
    for head in range(heads):
        load(("out", head), out_hbm.at[:, head], out_w.at[head])
    load("gate", gate_hbm.at[0], gate_w)
    load("up", up_hbm.at[0], up_w)
    load("down", down_hbm.at[0], down_w)

    for name in ("routing", "route", "queries"):
        loads[name].wait()
    own_weights = weights_all.at[sp, tp]
    own_weights[...] = jnp.zeros_like(own_weights)
    for expert in range(QUADS):
        row = 0.0
        for k in range(routing.shape[0]):
            row = row + jnp.where(
                routing[k : k + 1, :] == expert, route_w[k : k + 1, :], 0.0
            )
        own_weights[expert : expert + 1, :count] = row

    chunk = LANES
    for head in range(heads):
        for at in range(tokens // chunk):
            span = slice(at * chunk, (at + 1) * chunk)
            row = gate_all[sp, head : head + 1, span] * LOG2E
            qcol[head, span] = jnp.transpose(jnp.broadcast_to(row, (chunk, chunk)))[:, :1]

    halves = 2 if tokens % (2 * chunk) == 0 and tp_count % 2 == 0 else 1

    def attend(quad, head, diagonal, parts):
        cols = head_cols(head)

        def attend_chunk(j):
            start = j * chunk
            rows = pl.ds(start if isinstance(start, int) else pl.multiple_of(start, chunk), chunk)
            scores = lax.dot_general(
                queries[rows, cols],
                pair_all[quad, head, 0],
                (((1,), (1,)), ((), ())),
                preferred_element_type=jnp.float32,
            )
            query_gate = qcol[head, rows]
            key_gate = gate_all[quad, head : head + 1, :] * LOG2E
            scores = scores * (HD ** (-0.5) * LOG2E) - key_gate
            if diagonal:
                row_id = lax.broadcasted_iota(jnp.int32, scores.shape, 0) + start
                col_id = lax.broadcasted_iota(jnp.int32, scores.shape, 1)
                scores = jnp.where(col_id <= row_id, scores, masked_score)
            new_peak = jnp.max(scores, axis=1, keepdims=True) + query_gate
            if not diagonal:
                old_peak = peak[head, rows]
                new_peak = jnp.maximum(old_peak, new_peak)
            lifted = jnp.exp2(scores + (query_gate - new_peak))
            added = jnp.sum(lifted, axis=1, keepdims=True)
            product = jnp.dot(
                lifted.astype(jnp.bfloat16),
                pair_all[quad, head, 1],
                preferred_element_type=jnp.float32,
            )
            if not diagonal:
                rescale = jnp.exp2(old_peak - new_peak)
                added = weight_total[head, rows] * rescale + added
                product = weighted[head, rows] * rescale + product
            return rows, new_peak, added, product

        group = tokens // (halves * chunk)

        def attend_group(j):
            for rows, new_peak, added, product in [attend_chunk(j * group + at) for at in range(group)]:
                peak[head, rows] = new_peak
                weight_total[head, rows] = added
                weighted[head, rows] = product

        for part in parts:
            attend_group(part)

    def attend_earlier(quad, head, parts=tuple(range(halves))):
        @pl.when(quad < sp)
        def _():
            attend(quad, head, False, parts)

    def take_first(head):
        kv_landed(first, head)
        kv_send(first, head, to_second, 1)
        if head + 1 < heads:
            kv_send(sp, head + 1, to_second, 1)
        attend_earlier(first, head)

    def take_second(head):
        kv_landed(second, head)
        attend_earlier(second, head)

    def finish(head):
        kv_landed(far, head)
        span, blocks = tokens // halves, tp_count // halves
        for part in range(halves):
            attend_earlier(far, head, (part,))
            rows = pl.ds(part * span, span)
            attended = weighted[head, rows] * (1.0 / weight_total[head, rows])
            square = jnp.mean(attended * attended, axis=1, keepdims=True)
            normed = attended * lax.rsqrt(square + 1e-06) * gain[0:1, head_cols(head)]
            targets = range(part * blocks, (part + 1) * blocks)
            leaving[head, targets.start : targets.stop] = bf16(normed).reshape(blocks, count, HD)
            for target in targets:

                @pl.when(tp != target)
                def _(target=target):
                    send(
                        leaving.at[head, target],
                        incoming.at[head, tp],
                        out_send_sems.at[head],
                        out_recv_sems.at[head, z],
                        (sp, target),
                    )

        drain_later(leaving.at[head, 0 : tp_count - 1], out_send_sems.at[head])
        incoming[head, tp] = leaving[head, tp]

    z_level = levels[0]
    word(0)
    for head in range(heads):
        attend(sp, head, True, range(halves))
    for stage in range(depth - 1):
        hear(stage)
        if stage + 1 < depth - 1:
            word(stage + 1)
    for step in range(1, tp_count):
        target = (tp + step) % tp_count
        ref = weights_all.at[sp, tp]
        send(ref, ref, w_send_sems.at[0], w_recv_sems.at[QUADS], (sp, target))
    drain_later(weights_all.at[0, 0 : tp_count - 1], w_send_sems.at[0])
    loads["gain"].wait()
    take_first(0)
    take_second(0)
    for head in range(heads):
        if head + 1 < heads:
            take_first(head + 1)
        finish(head)
        if head + 1 < heads:
            take_second(head + 1)
    landed(weights_all.at[sp, 0 : tp_count - 1], w_recv_sems.at[QUADS])

    def spread_weights(quad, target):
        ref = weights_all.at[quad]
        send(ref, ref, w_send_sems.at[1], w_recv_sems.at[quad], target)

    spread_weights(sp, to_first)
    spread_weights(sp, to_second)
    drain_later(weights_all.at[0:3], w_send_sems.at[1])
    loads["stream"].wait()
    resid[...] = f32(stream[...])
    loads["norm"].wait()
    strip = 1024 if width % 1024 == 0 else width
    for head in range(heads):
        loads["out", head].wait()
        for level in levels:
            sources = (level * 2, level * 2 + 1)
            from_level = incoming.at[head, pl.ds(level * 2, 2)]
            if level is z_level:
                from_level = incoming.at[head, level * 2 + other]
            landed(from_level, out_recv_sems.at[head, level])

            @pl.loop(0, width // strip)
            def _(j, head=head, level=level, sources=sources):
                cols = pl.ds(pl.multiple_of(j * strip, strip), strip)
                rows = jnp.concatenate([incoming[head, source] for source in sources], axis=1)
                weights = out_w[head, pl.ds(level * 2, 2), :, cols].reshape(2 * HD, strip)
                resid[:, cols] += jnp.dot(rows, weights, preferred_element_type=jnp.float32)

    landed(weights_all.at[first], w_recv_sems.at[first])
    spread_weights(first, to_second)
    total = resid[...]
    center = total - jnp.mean(total, axis=1, keepdims=True)
    variance = jnp.mean(center * center, axis=1, keepdims=True)
    rows_all[core, z, sp] = (center * lax.rsqrt(variance + 1e-05) * norm_gain[0:1, :]).astype(
        jnp.bfloat16
    )

    ag_count = [3]

    def part_of(k):
        return pl.ds(k * part_rows, part_rows)

    def spread(level, quad, k, target, sem, recv_sem=None):
        ref = rows_all.at[core, level, quad, part_of(k)]
        if recv_sem is None:
            recv_sem = ag_recv_sems.at[level, quad, k]
        send(ref, ref, ag_send_sems.at[sem], recv_sem, target)

    def spread_all(level, quad, target, sem):
        for k in range(PARTS):
            spread(level, quad, k, target, sem)

    def to_partner(level, quad, k):
        spread(level, quad, k, to_core, 0, part_recv_sems.at[level])

    def lane_when(when):
        sem = ag_count[0]
        ag_count[0] += 1
        drain_later(rows_all.at[0, 0, 0], ag_send_sems.at[sem], when)

        def spread_when(level, quad, k, target):
            @pl.when(when)
            def _():
                spread(level, quad, k, target, sem)

        return spread_when

    def arrived(level, quad, k):
        landed(rows_all.at[core, level, quad, part_of(k)], ag_recv_sems.at[level, quad, k])

    drain_later(rows_all.at[0], ag_send_sems.at[0])
    drain_later(rows_all.at[0, 0:2], ag_send_sems.at[1])
    drain_later(rows_all.at[0, 0, 0], ag_send_sems.at[2])
    own_above, own_below = lane_when(z < depth - 1), lane_when(z > 0)
    for k in range(PARTS):
        own_above(z, sp, k, above)
        own_below(z, sp, k, below)
        spread(z, sp, k, to_first, 2)
        spread(z, sp, k, to_second, 1)
        to_partner(z, sp, k)

    landed(weights_all.at[second], w_recv_sems.at[second])
    landed(weights_all.at[far], w_recv_sems.at[far])
    lane = lax.broadcasted_iota(jnp.int32, (QUADS, LANES), 0)
    picked = []
    for quad in range(QUADS):
        for source in range(tp_count):
            tile = weights_all[quad, source]
            picked.append(jnp.sum(jnp.where(lane == sp, tile, 0.0), axis=0, keepdims=True))
    fill = jnp.zeros((LANES - len(picked), LANES), jnp.float32)
    turned = jnp.transpose(jnp.concatenate(picked + [fill], axis=0))
    for quad in range(QUADS):
        for source in range(tp_count):
            at = quad * tp_count + source
            wcols[source % 2, source // 2, quad] = turned[:count, at : at + 1]

    for name in ("gate", "up", "down"):
        loads[name].wait()

    def hidden_units(half, level):
        piece = 512 if units % 512 == 0 else units

        @pl.loop(0, units // piece)
        def _(j):
            cols = pl.ds(pl.multiple_of(j * piece, piece), piece)
            block = rows_all[half, level].reshape(QUADS * count, width)
            gate_pre = jnp.dot(block, gate_w[:, cols], preferred_element_type=jnp.float32)
            up_pre = jnp.dot(block, up_w[:, cols], preferred_element_type=jnp.float32)
            hidden[half, level, :, cols] = bf16(gate_pre / (1.0 + jnp.exp(-gate_pre)) * up_pre)

    def down_product(half, level, dest):
        piece = 1024 if width % 1024 == 0 else width

        @pl.loop(0, width // piece)
        def _(j):
            cols = pl.ds(pl.multiple_of(j * piece, piece), piece)
            weight = wcols[half, level].reshape(QUADS * count, 1)
            product = jnp.dot(hidden[half, level], down_w[:, cols], preferred_element_type=jnp.float32)
            dest[level, :, :, cols] = bf16(product * weight).reshape(QUADS, count, piece)

    def from_z_near(place):
        level = levels[place]
        go_above = lane_when((level < z) & (z < depth - 1))
        go_below = lane_when((level > z) & (z > 0))
        go_first = lane_when((level - z) * (level - z) != 1)
        for k in range(PARTS):
            arrived(level, sp, k)
            go_above(level, sp, k, above)
            go_below(level, sp, k, below)
            go_first(level, sp, k, to_first)
            spread(level, sp, k, to_second, 1)
            to_partner(level, sp, k)

    def from_first_near(place):
        level = levels[place]
        if place == 0:
            go_above, go_below = lane_when(z < depth - 1), lane_when(z > 0)
        for k in range(PARTS):
            arrived(level, first, k)
            if place == 0:
                go_above(level, first, k, above)
                go_below(level, first, k, below)
            spread(level, first, k, to_second, 1)
            to_partner(level, first, k)

    def from_second_near(place):
        for k in range(PARTS):
            arrived(levels[place], second, k)
            to_partner(levels[place], second, k)

    def from_far(place):
        for k in range(PARTS):
            arrived(levels[place], far, k)
            to_partner(levels[place], far, k)

    def send_back(src, dst, lane, sem, target, when=None):
        send(src, dst, rs_send_sems.at[lane], sem, target, when)

    drain_later(mine, rs_send_sems.at[0])
    drain_later(rows_all.at[0, 0:2], rs_send_sems.at[1])
    drain_later(rows_all.at[0, 0, 0:3], rs_send_sems.at[2])
    drain_later(rows_all.at[0, 0, 0], rs_send_sems.at[3])

    def own_hidden(place):
        hidden_units(core, levels[place])

    def own_product(place):
        down_product(core, levels[place], mine)

    def partner_hidden(place):
        level = levels[place]
        landed(rows_all.at[other, level], part_recv_sems.at[level])
        hidden_units(other, level)

    def partner_product(place):
        level = levels[place]
        down_product(other, level, theirs)
        send_back(theirs.at[level], from_core.at[level], 0, core_sems.at[level], to_core)

    def both_halves(place):
        level = levels[place]
        landed(from_core.at[level], core_sems.at[level])
        for slot, quad in ((1, far), (0, second)):
            for k in range(PARTS):
                rows = part_of(k)
                mine[level, quad, rows] = bf16(
                    f32(mine[level, quad, rows]) + f32(from_core[level, quad, rows])
                )
                send_back(
                    mine.at[level, quad, rows],
                    from_second.at[level, slot, rows],
                    1,
                    second_sems.at[level, slot, k],
                    to_second,
                )

    def onto_first(place):
        level = levels[place]
        if place == 0:
            for near in levels[1:]:

                @pl.when(adjacent(near))
                def _(near=near):
                    for k in range(PARTS):
                        rows = part_of(k)
                        landed(from_zf.at[near, rows], zf_sems.at[near, k])
                    mine[z, first] = bf16(f32(mine[z, first]) + f32(from_zf[near]))

        near, apart = adjacent(level), (level - z) * (level - z) != 1
        if place:
            drain_later(rows_all.at[0, 0, 0], rs_send_sems.at[2 + 2 * place], near)
            drain_later(rows_all.at[0, 0, 0], rs_send_sems.at[3 + 2 * place], apart)
        for k in range(PARTS):
            rows = part_of(k)
            landed(from_second.at[level, 1, rows], second_sems.at[level, 1, k])
            mine[level, first, rows] = bf16(
                f32(mine[level, first, rows])
                + f32(from_core[level, first, rows])
                + f32(from_second[level, 1, rows])
            )
            src = mine.at[level, first, rows]
            dst, sem = from_first.at[level, rows], first_sems.at[level, k]
            if place:
                zf_dst, zf_sem = from_zf.at[z, rows], zf_sems.at[z, k]
                send_back(src, zf_dst, 2 + 2 * place, zf_sem, at_z(level), near)
                send_back(src, dst, 3 + 2 * place, sem, to_first, apart)
            else:
                send_back(src, dst, 3, sem, to_first)

    def onto_owner(place):
        level = levels[place]
        for k in range(PARTS):
            rows = part_of(k)
            landed(from_second.at[level, 0, rows], second_sems.at[level, 0, k])

            def total_of(with_first, rows=rows):
                total = f32(mine[level, sp, rows]) + f32(from_core[level, sp, rows])
                total = total + f32(from_second[level, 0, rows])
                return total + f32(from_first[level, rows]) if with_first else total

            if place == 0:
                landed(from_first.at[level, rows], first_sems.at[level, k])
                resid[rows] += total_of(True)
                continue

            @pl.when((level - z) * (level - z) != 1)
            def _(k=k, rows=rows, total_of=total_of):
                landed(from_first.at[level, rows], first_sems.at[level, k])
                mine[level, sp, rows] = bf16(total_of(True))

            @pl.when(adjacent(level))
            def _(rows=rows, total_of=total_of):
                mine[level, sp, rows] = bf16(total_of(False))

            src = mine.at[level, sp, rows]
            send_back(src, from_z.at[z, rows], 2, z_sems.at[z, k], at_z(level))

    tasks = dict(
        zr=from_z_near,
        fa=from_first_near,
        s=from_second_near,
        d=from_far,
        co1=own_hidden,
        co2=own_product,
        cp1=partner_hidden,
        cp2=partner_product,
        r1=both_halves,
        r2=onto_first,
        r3=onto_owner,
    )
    for name, place in TASKS:
        tasks[name](place)

    total = resid[...]
    for near in levels[1:]:
        for k in range(PARTS):
            landed(from_z.at[near, part_of(k)], z_sems.at[near, k])
        total = total + f32(from_z[near])
    out_ref[...] = total.astype(out_ref.dtype)

    def drain(ref, sem):
        pltpu.make_async_remote_copy(
            src_ref=ref,
            dst_ref=ref,
            send_sem=sem,
            recv_sem=kv_recv_sems.at[0, 0],
            device_id=to_core,
            device_id_type=MESH,
        ).wait_send()

    for ref, sem, when in drains:
        if when is None:
            drain(ref, sem)
        else:
            pl.when(when)(partial(drain, ref, sem))


def whole_layer(
    queries,
    keys,
    values,
    forget_totals,
    head_gain,
    stream,
    out_weight,
    norm_gain,
    routing,
    route_weights,
    gate_weight,
    up_weight,
    down_weight,
):
    tokens, wide = queries.shape
    heads = wide // HD
    count, width = stream.shape
    units = gate_weight.shape[2]
    tp_count = lax.axis_size("tp")
    depth = tp_count // 2
    top = routing.shape[1]
    bf16, f32 = jnp.bfloat16, jnp.float32
    dma = pltpu.SemaphoreType.DMA
    vmem = pltpu.VMEM
    plane = (depth, QUADS, count, width)
    hbm = pl.BlockSpec(memory_space=pltpu.HBM)
    return pl.pallas_call(
        partial(layer_kernel, depth),
        out_shape=jax.ShapeDtypeStruct((count, width), bf16),
        in_specs=[hbm] * 13,
        out_specs=pl.BlockSpec(memory_space=pltpu.VMEM),
        scratch_shapes=[
            vmem((tokens, wide), bf16),
            vmem((count, width), bf16),
            vmem((1, wide), f32),
            vmem((1, width), f32),
            vmem((top, count), jnp.int32),
            vmem((top, count), f32),
            vmem((QUADS, heads, 2, tokens, HD), bf16),
            vmem((QUADS, heads, tokens), f32),
            vmem((QUADS, tp_count, QUADS, LANES), f32),
            vmem((2, depth, QUADS, count, 1), f32),
            vmem((heads, tokens, 1), f32),
            vmem((heads, tokens, 1), f32),
            vmem((heads, tokens, 1), f32),
            vmem((heads, tokens, HD), f32),
            vmem((heads, tp_count, count, HD), bf16),
            vmem((heads, tp_count, count, HD), bf16),
            vmem((count, width), f32),
            vmem((heads, tp_count, HD, width), bf16),
            vmem((2,) + plane, bf16),
            vmem((width, units), bf16),
            vmem((width, units), bf16),
            vmem((units, width), bf16),
            vmem((2, depth, QUADS * count, units), bf16),
            vmem(plane, bf16),
            vmem(plane, bf16),
            vmem(plane, bf16),
            vmem((depth, 2, count, width), bf16),
            vmem((depth, count, width), bf16),
            vmem((depth, count, width), bf16),
            vmem((depth, count, width), bf16),
            pltpu.SemaphoreType.REGULAR((depth - 1, 3)),
            dma((10 + 3 * heads,)),
            dma((3,)),
            dma((QUADS, heads + 1)),
            dma((heads,)),
            dma((heads, depth)),
            dma((2,)),
            dma((QUADS + 1,)),
            dma((3 + 2 + 2 + 3 * (depth - 1),)),
            dma((depth, QUADS, PARTS)),
            dma((depth,)),
            dma((2 + 2 * depth,)),
            dma((depth,)),
            dma((depth, 2, PARTS)),
            dma((depth, PARTS)),
            dma((depth, PARTS)),
            dma((depth, PARTS)),
        ],
        compiler_params=pltpu.CompilerParams(
            collective_id=0, has_side_effects=True, vmem_limit_bytes=50 * 2**20
        ),
    )(
        *(
            pltpu.with_memory_space_constraint(operand, pltpu.HBM)
            for operand in (
                queries,
                keys,
                values,
                jnp.transpose(forget_totals),
                head_gain.reshape(1, -1),
                stream,
                out_weight.reshape(tp_count, heads, HD, width),
                norm_gain.reshape(1, -1),
                jnp.transpose(routing),
                jnp.transpose(route_weights),
                gate_weight,
                up_weight,
                down_weight,
            )
        )
    )


def routed_experts(
    resid_sum, normed_rows, routing, route_weights, gate_weight, up_weight, down_weight
):
    sp_count = lax.axis_size("sp")
    row_count = normed_rows.shape[0]
    capacity = max(2, 2 * TOP * row_count // sp_count)
    flat_expert = routing.reshape(-1)
    onehot = (flat_expert[:, None] == jnp.arange(sp_count, dtype=jnp.int32)[None, :]).astype(
        jnp.int32
    )
    earlier = jnp.cumsum(onehot, axis=0) - onehot
    slot_index = flat_expert * capacity + jnp.sum(earlier * onehot, axis=1)
    slot_grid = slot_index.reshape(row_count, TOP)
    slot_ids = jnp.arange(sp_count * capacity, dtype=jnp.int32)
    placing = jnp.sum(
        (slot_grid[None, :, :] == slot_ids[:, None, None]).astype(jnp.float32), axis=2
    ).astype(jnp.bfloat16)
    outgoing = jnp.dot(placing, normed_rows, preferred_element_type=jnp.float32).astype(
        jnp.bfloat16
    )
    outgoing = outgoing.reshape(sp_count, capacity, normed_rows.shape[1])
    arrived = lax.all_to_all(outgoing, "sp", split_axis=0, concat_axis=0, tiled=True)
    row_piece = lax.all_gather(arrived.reshape(-1, arrived.shape[2]), "tp", axis=0, tiled=True)
    gate_pre = jnp.dot(row_piece, gate_weight[0], preferred_element_type=jnp.float32)
    up_pre = jnp.dot(row_piece, up_weight[0], preferred_element_type=jnp.float32)
    hidden = (jax.nn.silu(gate_pre) * up_pre).astype(jnp.bfloat16)
    summed = lax.psum_scatter(
        jnp.dot(hidden, down_weight[0], preferred_element_type=jnp.float32).astype(jnp.bfloat16),
        "tp",
        scatter_dimension=0,
        tiled=True,
    )
    expert_out = summed.reshape(sp_count, capacity, -1)
    returned = lax.all_to_all(expert_out, "sp", split_axis=0, concat_axis=0, tiled=True)
    picked = returned.reshape(sp_count * capacity, -1)[slot_index].astype(jnp.float32)
    weighted = picked * route_weights.reshape(-1)[:, None]
    routed = jnp.sum(weighted.reshape(row_count, TOP, -1), axis=1)
    return (resid_sum + routed).astype(jnp.bfloat16)


def on_device(
    queries,
    key_vectors,
    value_vectors,
    forget_totals,
    head_gain,
    stream,
    out_weight,
    norm_gain,
    routing,
    route_weights,
    gate_weight,
    up_weight,
    down_weight,
):
    rows_dev, sp_size, tp_size = stream.shape[0], lax.axis_size("sp"), lax.axis_size("tp")
    dense = 2 * TOP * rows_dev // sp_size >= rows_dev
    leveled = sp_size == QUADS and tp_size == 2 * len({place for _, place in TASKS})
    if dense and leveled and queries.shape[0] % LANES == 0 and rows_dev <= LANES and rows_dev % (16 * PARTS) == 0:
        return whole_layer(
            queries,
            key_vectors,
            value_vectors,
            forget_totals,
            head_gain,
            stream,
            out_weight,
            norm_gain,
            routing,
            route_weights,
            gate_weight,
            up_weight,
            down_weight,
        )
    tok_count = queries.shape[0]
    heads_dev = queries.shape[1] // HD
    sp_index = lax.axis_index("sp")
    sp_count = lax.axis_size("sp")
    gathered_gates = lax.all_gather(forget_totals, "sp", axis=0, tiled=True)
    first_pos = sp_index * tok_count
    query_pos = first_pos + jnp.arange(tok_count, dtype=jnp.int32)
    query_gate = jnp.transpose(lax.dynamic_slice_in_dim(gathered_gates, first_pos, tok_count, 0))
    segments = [(queries.reshape(tok_count, heads_dev, HD), query_gate, query_pos)]
    starting = (
        (
            jnp.full((heads_dev, tok_count), masked_score, jnp.float32),
            jnp.zeros((heads_dev, tok_count), jnp.float32),
            jnp.zeros((heads_dev, tok_count, HD), jnp.float32),
        ),
    )
    folder = make_folder(segments, gathered_gates)
    totals = folder(
        starting,
        (
            lax.all_gather(key_vectors, "sp", axis=0, tiled=True),
            lax.all_gather(value_vectors, "sp", axis=0, tiled=True),
        ),
        jnp.int32(0),
    )
    run_max, run_sum, run_acc = totals[0]
    attended = run_acc / run_sum[:, :, None]
    inverse_rms = lax.rsqrt(jnp.mean(attended * attended, axis=2, keepdims=True) + 1e-06)
    normed = attended * inverse_rms * head_gain.reshape(heads_dev, 1, HD)
    head_out = (
        jnp.transpose(normed, (1, 0, 2)).reshape(tok_count, heads_dev * HD).astype(jnp.bfloat16)
    )
    token_heads = lax.all_to_all(head_out, "tp", split_axis=0, concat_axis=1, tiled=True)
    mixed_rows = jnp.dot(token_heads, out_weight, preferred_element_type=jnp.float32)
    resid_sum = stream.astype(jnp.float32) + mixed_rows
    center = resid_sum - jnp.mean(resid_sum, axis=1, keepdims=True)
    normed_rows = (
        center * lax.rsqrt(jnp.mean(center * center, axis=1, keepdims=True) + 1e-05) * norm_gain
    ).astype(jnp.bfloat16)
    return routed_experts(
        resid_sum, normed_rows, routing, route_weights, gate_weight, up_weight, down_weight
    )


def solution(mesh):
    in_specs = (
        P("sp", "tp"),
        P("sp", "tp"),
        P("sp", "tp"),
        P("sp", "tp"),
        P("tp"),
        P(("sp", "tp"), None),
        P(),
        P(),
        P(("sp", "tp"), None),
        P(("sp", "tp"), None),
        P("sp", None, "tp"),
        P("sp", None, "tp"),
        P("sp", "tp", None),
    )
    out_specs = P(("sp", "tp"), None)
    return jax.shard_map(
        on_device, mesh=mesh, in_specs=in_specs, out_specs=out_specs, check_vma=False
    )
```
